32 devices in a mesh: sp: 8 (over z, x), tp: 4 (over y, core).
Axes of the slice: x: 2, y: 2, z: 4, core: 2. Of those that a mesh axis runs over, the one named last changes fastest.
Arguments:
- tokens: bfloat16 [8192, 2048], P('sp'), may hold values from -8 to 8
- norm_gain: float32 [2048], replicated, may hold values from 0.1 to 1.9
- query_weight: bfloat16 [2048, 512], P(None, 'tp'), may hold values from -40 to 40
- key_weight: bfloat16 [2048, 256], P(None, 'tp'), may hold values from -1 to 1
- value_weight: bfloat16 [2048, 256], P(None, 'tp'), may hold values from -0.125 to 0.125
- sink_logits: float32 [8], P('tp'), may hold values from 1 to 6
- conv_in_weight: bfloat16 [2048, 512], P(None, 'tp'), may hold values from -0.125 to 0.125
- conv_gate_weight: bfloat16 [2048, 512], P(None, 'tp'), may hold values from -0.125 to 0.125
- conv_taps: bfloat16 [31, 512], replicated, may hold values from -1 to 1
- conv_gain: float32 [512], replicated, may hold values from 0.1 to 1.9
- point_weight: bfloat16 [512, 512], replicated, may hold values from -0.25 to 0.25
- output_gain: float32 [1024], replicated, may hold values from 0.1 to 1.9
- output_weight: bfloat16 [1024, 2048], P('sp'), may hold values from -0.1875 to 0.1875
Outputs:
- mixed_output: bfloat16 [8192, 2048], P(('sp', 'tp'))
The draws below stay inside these ranges and needn't reach their ends.
All inputs are finite; a program needn't handle non-finite values.
Results may differ from the reference program's by a relative error of at most 0.0087.
Values may be sent and summed in bfloat16 or wider, within the bound.
No kernel may reach another device: no remote copies, remote signals or barrier semaphores. Data moves between devices by JAX's collectives and lax.ppermute only.
A program may use at most 64 MiB of HBM per device.

```python
import jax
import jax.numpy as jnp
from jax import lax

D = 2048
HEADS = 8
KV_HEADS = 4
HEAD_DIM = 64
CHANNELS = 512
WINDOW = 128
CONV_WIDTH = 31
TOKENS = 8192
MIX = 1024


def base_query(key):
    gaussian = jax.random.normal(jax.random.fold_in(key, 501), (D, HEADS * HEAD_DIM), jnp.float32)
    return jnp.clip(gaussian, -6.0, 6.0) * D ** (-0.5)


def draw_query_weight(key, part):
    unscaled = base_query(key)
    return unscaled.astype(jnp.bfloat16)


def draw_key_weight(key, part):
    fresh_noise = jax.random.normal(jax.random.fold_in(key, 502), (D, KV_HEADS * HEAD_DIM), jnp.float32)
    fresh_noise = jnp.clip(fresh_noise, -6.0, 6.0) * D ** (-0.5)
    return fresh_noise.astype(jnp.bfloat16)


def draw_tokens(key, part):
    shape_rows = (TOKENS, D)
    gaussian = jnp.clip(jax.random.normal(jax.random.fold_in(key, 601), shape_rows, jnp.float32), -6.0, 6.0)
    return gaussian.astype(jnp.bfloat16)


def block_levels(key, extent, split, low, top_value):
    def one(dim, shards_of):
        heights = jax.random.uniform(jax.random.fold_in(jax.random.fold_in(key, 6), dim), (shards_of,), jnp.float32, low / len(split), top_value / len(split))
        return jnp.repeat(jnp.exp(heights), extent[dim] // shards_of).reshape((-1,) + (1,) * (len(extent) - dim - 1))

    factor_of = one(*split[0])
    for cut in split[1:]:
        factor_of = factor_of * one(*cut)
    return factor_of


def scatter_about(key, dims, deviation, reach, cuts=(), kind=jnp.bfloat16):
    entries = deviation * jax.random.normal(key, dims, jnp.float32)
    if cuts:
        entries = entries * block_levels(key, dims, cuts, -0.22, 0.18)
    return jnp.clip(entries, -reach, reach).astype(kind)


def setup_inputs(seed: int = 0) -> dict:
    seeds = jax.random.split(jax.random.key(seed), 14)
    return {
        "tokens": draw_tokens(jax.random.fold_in(seeds[13], 71), 0),
        "norm_gain": jnp.clip(1.0 + 0.18 * jax.random.normal(seeds[1], (D,), jnp.float32), 0.1, 1.9),
        "query_weight": draw_query_weight(jax.random.fold_in(seeds[13], 71), 0),
        "key_weight": draw_key_weight(jax.random.fold_in(seeds[13], 71), 0),
        "value_weight": scatter_about(seeds[4], (D, KV_HEADS * HEAD_DIM), D ** -0.5, 0.125, ((1, 4),)),
        "sink_logits": jnp.clip(1.0 + 5.0 * jax.random.uniform(seeds[5], (HEADS,), jnp.float32) ** block_levels(seeds[5], (HEADS,), ((0, 4),), -0.2, 0.2), 1.0, 6.0),
        "conv_in_weight": scatter_about(seeds[6], (D, CHANNELS), D ** -0.5, 0.125, ((1, 4),)),
        "conv_gate_weight": scatter_about(seeds[7], (D, CHANNELS), D ** -0.5, 0.125, ((1, 4),)),
        "conv_taps": scatter_about(seeds[8], (CONV_WIDTH, CHANNELS), CONV_WIDTH ** -0.5, 1.0),
        "conv_gain": jnp.clip(1.0 + 0.18 * jax.random.normal(seeds[9], (CHANNELS,), jnp.float32), 0.1, 1.9),
        "point_weight": scatter_about(seeds[10], (CHANNELS, CHANNELS), CHANNELS ** -0.5, 0.25),
        "output_gain": jnp.clip(1.0 + 0.18 * jax.random.normal(seeds[11], (MIX,), jnp.float32), 0.1, 1.9),
        "output_weight": scatter_about(seeds[12], (MIX, D), MIX ** -0.5, 0.1875, ((0, 8),)),
    }


NORM_EPSILON = 1e-06
MASKED_SCORE = -1e+30

def rms_rows(values, scale_gain):
    return values * lax.rsqrt(lax.optimization_barrier(jnp.mean(values * values, axis=-1, keepdims=True)) + NORM_EPSILON) * scale_gain

def depthwise(current, earlier_rows, tap_weights):
    extended = jnp.concatenate([earlier_rows, current], axis=0).astype(jnp.float32)
    tap_floats = tap_weights.astype(jnp.float32)
    row_count = current.shape[0]
    result = jnp.zeros(current.shape, jnp.float32)
    for tap_index in range(CONV_WIDTH):
        result = result + tap_floats[tap_index] * extended[tap_index:tap_index + row_count]
    return lax.optimization_barrier(result.astype(jnp.bfloat16))

def layer_activate(conv_rows, channel_gain):
    widened = conv_rows.astype(jnp.float32)
    centered = widened - lax.optimization_barrier(jnp.mean(widened, axis=-1, keepdims=True))
    scaled = centered * lax.rsqrt(lax.optimization_barrier(jnp.mean(centered * centered, axis=-1, keepdims=True)) + NORM_EPSILON) * channel_gain
    return jax.nn.silu(scaled).astype(jnp.bfloat16)

def merge_groups(attended, pointwise, output_gain):
    head_width = attended.shape[1]
    return jnp.concatenate([rms_rows(attended.astype(jnp.float32), output_gain[:head_width]), rms_rows(pointwise, output_gain[head_width:])], axis=1).astype(jnp.bfloat16)

def reference(tokens, norm_gain, query_weight, key_weight, value_weight, sink_logits, conv_in_weight, conv_gate_weight, conv_taps, conv_gain, point_weight, output_gain, output_weight):
    normed = rms_rows(tokens.astype(jnp.float32), norm_gain).astype(jnp.bfloat16)
    queries = jnp.dot(normed, query_weight, preferred_element_type=jnp.float32).astype(jnp.bfloat16)
    key_part = jnp.dot(normed, key_weight, preferred_element_type=jnp.float32).astype(jnp.bfloat16)
    value_part = jnp.dot(normed, value_weight, preferred_element_type=jnp.float32).astype(jnp.bfloat16)
    conv_in = jnp.dot(normed, conv_in_weight, preferred_element_type=jnp.float32)
    conv_gate = jnp.dot(normed, conv_gate_weight, preferred_element_type=jnp.float32)
    gated_rows = (conv_in * jax.nn.sigmoid(conv_gate)).astype(jnp.bfloat16)
    group_size = HEADS // KV_HEADS
    block_count = TOKENS // WINDOW
    head_queries = jnp.transpose(queries.reshape(TOKENS, KV_HEADS, group_size, HEAD_DIM), (1, 0, 2, 3))
    head_keys = jnp.transpose(key_part.reshape(TOKENS, KV_HEADS, HEAD_DIM), (1, 0, 2))
    head_values = jnp.transpose(value_part.reshape(TOKENS, KV_HEADS, HEAD_DIM), (1, 0, 2))
    head_sinks = sink_logits.reshape(KV_HEADS, group_size)
    query_index = lax.broadcasted_iota(jnp.int32, (WINDOW, 2 * WINDOW), 0)
    key_index = lax.broadcasted_iota(jnp.int32, (WINDOW, 2 * WINDOW), 1)
    distance = WINDOW + query_index - key_index
    in_window = (distance >= 0) & (distance < WINDOW)
    block_start = jnp.arange(block_count, dtype=jnp.int32) * WINDOW - WINDOW
    allowed = in_window[None] & (block_start[:, None, None] + key_index[None] >= 0)

    def banded(rows_in):
        padding = jnp.zeros((WINDOW, HEAD_DIM), rows_in.dtype)
        extended = jnp.concatenate([padding, rows_in], axis=0).reshape(block_count + 1, WINDOW, HEAD_DIM)
        return jnp.concatenate([extended[:-1], extended[1:]], axis=1)

    def one_head(operands):
        group_queries, group_keys, group_values, group_sinks = operands
        blocked = group_queries.reshape(block_count, WINDOW, group_size, HEAD_DIM).astype(jnp.float32)
        scores = jnp.einsum('nqgd,njd->ngqj', blocked, banded(group_keys).astype(jnp.float32)) * HEAD_DIM ** (-0.5)
        scores = jnp.where(allowed[:, None], scores, MASKED_SCORE)
        sink_logit = group_sinks[None, :, None, None]
        row_peak = jnp.maximum(lax.optimization_barrier(jnp.max(scores, axis=-1, keepdims=True)), sink_logit)
        raised = jnp.exp(scores - row_peak)
        denominator = lax.optimization_barrier(jnp.sum(raised, axis=-1, keepdims=True)) + jnp.exp(sink_logit - row_peak)
        weights = (raised / denominator).astype(jnp.bfloat16)
        attended = jnp.einsum('ngqj,njd->nqgd', weights.astype(jnp.float32), banded(group_values).astype(jnp.float32))
        return attended.astype(jnp.bfloat16)
    per_head = lax.map(one_head, (head_queries, head_keys, head_values, head_sinks))
    attended = jnp.transpose(per_head, (1, 2, 0, 3, 4)).reshape(TOKENS, HEADS * HEAD_DIM)
    earlier_rows = jnp.zeros((CONV_WIDTH - 1, CHANNELS), jnp.bfloat16)
    convolved = depthwise(gated_rows, earlier_rows, conv_taps)
    activated = layer_activate(convolved, conv_gain)
    pointwise = jnp.dot(activated, point_weight, preferred_element_type=jnp.float32)
    merged = merge_groups(attended, pointwise, output_gain)
    return jnp.dot(merged, output_weight, preferred_element_type=jnp.float32).astype(jnp.bfloat16)
```

```python
import jax
import jax.numpy as jnp
from jax import lax
from jax.experimental import pallas as pl
from jax.experimental.pallas import tpu as pltpu
from jax.sharding import PartitionSpec as P

HEADS = 8
KV_HEADS = 4
HEAD_DIM = 64
WINDOW = 128
CONV_WIDTH = 31


NORM_EPSILON = 1e-06
MASKED_SCORE = -1e30


PLACE = ("sp", "tp")


def from_behind(block, axis, distance):
    devices = range(lax.axis_size(axis))
    route = [(i - distance, i) for i in devices if i - distance in devices]
    return lax.ppermute(block, axis, route)


def rms_rows(values, scale_gain):
    return (
        values
        * lax.rsqrt(jnp.mean(values * values, axis=-1, keepdims=True) + NORM_EPSILON)
        * scale_gain
    )


def depthwise(current, earlier_rows, tap_weights):
    extended = jnp.concatenate([earlier_rows, current], axis=0).astype(jnp.float32)
    tap_floats = tap_weights.astype(jnp.float32)
    row_count = current.shape[0]
    result = jnp.zeros(current.shape, jnp.float32)
    for tap_index in range(CONV_WIDTH):
        result = result + tap_floats[tap_index] * extended[tap_index : tap_index + row_count]
    return lax.optimization_barrier(result.astype(jnp.bfloat16))


def layer_activate(conv_rows, channel_gain):
    widened = conv_rows.astype(jnp.float32)
    centered = widened - jnp.mean(widened, axis=-1, keepdims=True)
    scaled = (
        centered
        * lax.rsqrt(jnp.mean(centered * centered, axis=-1, keepdims=True) + NORM_EPSILON)
        * channel_gain
    )
    return jax.nn.silu(scaled).astype(jnp.bfloat16)


def merge_groups(attended, pointwise, output_gain):
    head_width = attended.shape[1]
    return jnp.concatenate(
        [
            rms_rows(attended.astype(jnp.float32), output_gain[:head_width]),
            rms_rows(pointwise, output_gain[head_width:]),
        ],
        axis=1,
    ).astype(jnp.bfloat16)


def window_attention(queries, key_values, earlier_pairs, sinks_here, offset):
    row_count = queries.shape[0]
    block_count = row_count // WINDOW
    group_size = HEADS // KV_HEADS
    key_heads = key_values.shape[1] // (2 * HEAD_DIM)
    extended = jnp.concatenate([earlier_pairs, key_values], axis=0)
    extended = extended.reshape(block_count + 1, WINDOW, 2, key_heads, HEAD_DIM)
    key_value_band = jnp.concatenate([extended[:-1], extended[1:]], axis=1)
    key_band = key_value_band[:, :, 0]
    value_band = key_value_band[:, :, 1]
    grouped = queries.reshape(block_count, WINDOW, key_heads, group_size, HEAD_DIM)
    scores = jnp.einsum(
        "nqkgd,njkd->nkgqj", grouped, key_band, preferred_element_type=jnp.float32
    ) * HEAD_DIM ** (-0.5)
    query_index = lax.broadcasted_iota(jnp.int32, (WINDOW, 2 * WINDOW), 0)
    key_index = lax.broadcasted_iota(jnp.int32, (WINDOW, 2 * WINDOW), 1)
    distance = WINDOW + query_index - key_index
    in_window = (distance >= 0) & (distance < WINDOW)
    block_start = offset + jnp.arange(block_count, dtype=jnp.int32) * WINDOW - WINDOW
    allowed = in_window[None] & (block_start[:, None, None] + key_index[None] >= 0)
    scores = jnp.where(allowed[:, None, None], scores, MASKED_SCORE)
    sink_logit = sinks_here.reshape(key_heads, group_size)[None, :, :, None, None]
    row_peak = jnp.maximum(jnp.max(scores, axis=-1, keepdims=True), sink_logit)
    raised = jnp.exp(scores - row_peak)
    denominator = jnp.sum(raised, axis=-1, keepdims=True) + jnp.exp(sink_logit - row_peak)
    weights = (raised / denominator).astype(jnp.bfloat16)
    attended = jnp.einsum(
        "nkgqj,njkd->nqkgd", weights, value_band, preferred_element_type=jnp.float32
    )
    return attended.astype(jnp.bfloat16).reshape(row_count, key_heads * group_size * HEAD_DIM)


def gather_shares(share, lines, tp_size):
    def number(line, side, lane):
        return (line * 2 + side) * tp_size + lane

    def route(target):
        found = []
        for line in range(lines):
            for side in range(2):
                for lane in range(tp_size):
                    to_line, to_side, to_lane = target(line, side, lane)
                    if 0 <= to_line < lines:
                        found.append((number(line, side, lane), number(to_line, to_side, to_lane)))
        return found

    def along(distance):
        def target(line, side, lane):
            to_line = line + distance if lane % 2 == 0 else line - distance
            swap = distance == lines - 1 and distance > 1
            return to_line, side, (lane ^ 1 if swap else lane)

        return target

    across = route(lambda line, side, lane: (line, 1 - side, lane))
    lanes = route(lambda line, side, lane: (line, side, lane ^ 1))

    position = lax.axis_index("sp")
    line, side = position // 2, position % 2
    lane = lax.axis_index("tp") % 2

    def source(distance, my_lane):
        swap = distance == lines - 1 and distance > 1
        sender = 1 - my_lane if swap else my_lane
        from_line = jnp.where(sender == 0, line - distance, line + distance)
        valid = (from_line >= 0) & (from_line < lines)
        return jnp.where(valid, from_line, -1)

    def share_index(from_line, at_side):
        return jnp.where(from_line >= 0, from_line * 2 + at_side, -1)

    lower_half = route(
        lambda line, side, lane: (line, 1 - side, lane) if lane % 2 == 0 else (-1, 0, 0)
    )
    reached = [lax.ppermute(share, PLACE, route(along(1)))]
    opposite = lax.ppermute(share, PLACE, lower_half)
    reached += [lax.ppermute(share, PLACE, route(along(d))) for d in range(2, lines)]
    traded = [lax.ppermute(piece, PLACE, across) for piece in reached]

    def near_index(at_lane):
        from_line = source(1, at_lane)
        return [
            jnp.where(at_lane == 0, line * 2 + 1 - side, -1),
            share_index(from_line, side),
            share_index(from_line, 1 - side),
        ]

    def far_index(at_lane):
        from_line = source(2, at_lane)
        for distance in range(3, lines):
            from_line = jnp.maximum(from_line, source(distance, at_lane))
        return [share_index(from_line, side), share_index(from_line, 1 - side)]

    near = jnp.concatenate([opposite, reached[0], traded[0]], axis=0)
    groups = [share, near, lax.ppermute(near, PLACE, lanes)]
    index = [[position], near_index(lane), near_index(1 - lane)]
    if lines > 2:
        far = jnp.concatenate([sum(reached[1:]), sum(traded[1:])], axis=0)
        groups += [far, lax.ppermute(far, PLACE, lanes)]
        index += [far_index(lane), far_index(1 - lane)]
    return groups, jnp.stack(sum(index, [])).astype(jnp.int32)


def project_pieces(merged, groups, index, share_rows):
    rows, width = merged.shape
    columns = groups[0].shape[1]
    places = [
        (group, part)
        for group, array in enumerate(groups)
        for part in range(array.shape[0] // share_rows)
    ]
    count = len(groups)

    def body(index_ref, merged_ref, *refs):
        group_refs, out_ref = refs[:count], refs[count]
        whole, arrived = refs[count + 1], refs[count + 2]

        def fill(slot):
            group, part = places[slot]
            start = pl.multiple_of(index_ref[slot] * share_rows, share_rows)
            return pltpu.make_async_copy(
                group_refs[group].at[pl.ds(part * share_rows, share_rows)],
                whole.at[pl.ds(start, share_rows)],
                arrived.at[slot],
            )

        for slot in range(len(places)):

            @pl.when(index_ref[slot] >= 0)
            def _():
                fill(slot).start()

        for slot in range(len(places)):

            @pl.when(index_ref[slot] >= 0)
            def _():
                fill(slot).wait()

        out_ref[...] = jnp.dot(
            merged_ref[...], whole[...], preferred_element_type=jnp.float32
        ).astype(out_ref.dtype)

    return pl.pallas_call(
        body,
        out_shape=jax.ShapeDtypeStruct((rows, columns), jnp.bfloat16),
        grid_spec=pltpu.PrefetchScalarGridSpec(
            num_scalar_prefetch=1,
            grid=(1,),
            in_specs=[pl.BlockSpec((rows, width), lambda i, s: (0, 0))]
            + [pl.BlockSpec(memory_space=pl.ANY)] * count,
            out_specs=pl.BlockSpec((rows, columns), lambda i, s: (0, 0)),
            scratch_shapes=[
                pltpu.VMEM((width, columns), jnp.bfloat16),
                pltpu.SemaphoreType.DMA((len(places),)),
            ],
        ),
        name="project_pieces",
    )(index, merged, *groups)


def on_device(
    tokens,
    norm_gain,
    query_weight,
    key_weight,
    value_weight,
    sink_logits,
    conv_in_weight,
    conv_gate_weight,
    conv_taps,
    conv_gain,
    point_weight,
    output_gain,
    output_weight,
):
    local_rows = tokens.shape[0]
    offset = lax.axis_index("sp") * local_rows
    sp_size, tp_size = lax.axis_size("sp"), lax.axis_size("tp")
    by_pieces = sp_size % 2 == 0 and tp_size % 2 == 0 and 2 <= sp_size // 2 <= 4
    if by_pieces:
        groups, index = gather_shares(output_weight, sp_size // 2, tp_size)
    normed = rms_rows(tokens.astype(jnp.float32), norm_gain).astype(jnp.bfloat16)
    queries = jnp.dot(normed, query_weight, preferred_element_type=jnp.float32).astype(jnp.bfloat16)
    key_part = jnp.dot(normed, key_weight, preferred_element_type=jnp.float32).astype(jnp.bfloat16)
    value_part = jnp.dot(normed, value_weight, preferred_element_type=jnp.float32).astype(
        jnp.bfloat16
    )
    key_values = jnp.concatenate([key_part, value_part], axis=1)
    conv_in = jnp.dot(normed, conv_in_weight, preferred_element_type=jnp.float32)
    conv_gate = jnp.dot(normed, conv_gate_weight, preferred_element_type=jnp.float32)
    gated_rows = (conv_in * jax.nn.sigmoid(conv_gate)).astype(jnp.bfloat16)
    earlier_pairs = from_behind(key_values[local_rows - WINDOW :], "sp", 1)
    attended = window_attention(queries, key_values, earlier_pairs, sink_logits, offset)
    head_rows, second_rows = (
        lax.all_to_all(attended, "tp", split_axis=0, concat_axis=1, tiled=True),
        lax.all_to_all(gated_rows, "tp", split_axis=0, concat_axis=1, tiled=True),
    )
    quarter_rows = second_rows.shape[0]
    earlier_quarter = from_behind(second_rows[quarter_rows - (CONV_WIDTH - 1) :], ("sp", "tp"), 1)
    conv_result = depthwise(second_rows, earlier_quarter, conv_taps)
    activated = layer_activate(conv_result, conv_gain)
    pointwise = jnp.dot(activated, point_weight, preferred_element_type=jnp.float32)
    merged = merge_groups(head_rows, pointwise, output_gain)
    if by_pieces:
        return project_pieces(merged, groups, index, output_weight.shape[0])
    projected = jnp.dot(
        merged,
        lax.all_gather(output_weight, "sp", axis=0, tiled=True),
        preferred_element_type=jnp.float32,
    )
    return projected.astype(jnp.bfloat16)


def solution(mesh):
    in_specs = (
        P("sp", None),
        P(),
        P(None, "tp"),
        P(None, "tp"),
        P(None, "tp"),
        P("tp"),
        P(None, "tp"),
        P(None, "tp"),
        P(),
        P(),
        P(),
        P(),
        P("sp", None),
    )
    out_specs = P(("sp", "tp"), None)
    return jax.shard_map(
        on_device, mesh=mesh, in_specs=in_specs, out_specs=out_specs, check_vma=False
    )
```

```python
import jax
import jax.numpy as jnp
from jax import lax
from jax.experimental import pallas as pl
from jax.experimental.pallas import tpu as pltpu
from jax.sharding import PartitionSpec as P


HEAD_DIM = 64
WINDOW = 128
CONV_WIDTH = 31


NORM_EPSILON = 1e-06
MASKED_SCORE = -1e30
HALO = 32


PLACE = ("sp", "tp")


def from_behind(block, axis, distance):
    devices = range(lax.axis_size(axis))
    route = [(i - distance, i) for i in devices if i - distance in devices]
    return lax.ppermute(block, axis, route)


def project_inputs(tokens, norm_gain, query_weight, key_weight, value_weight, in_weight, gate_weight):
    rows, width = tokens.shape
    heads_width, pair_width = query_weight.shape[1], key_weight.shape[1] + value_weight.shape[1]
    key_width, channels = key_weight.shape[1], in_weight.shape[1]
    block = 256
    blocks = rows // block
    tail = WINDOW + HALO
    starts = [0, heads_width + pair_width, heads_width + pair_width + channels]

    def body(
        gain_hbm, tokens_hbm, query_hbm, key_hbm, value_hbm, in_hbm, gate_hbm,
        queries_ref, pairs_ref, gated_ref, tail_ref,
        fetched, normed, joined, pairs_rows, gain_ref, arrived, fetched_sem,
    ):
        fetches = [
            pltpu.make_async_copy(
                tokens_hbm.at[pl.ds(i * block, block)], fetched.at[i], fetched_sem.at[i]
            )
            for i in range(blocks)
        ]
        copies = [
            pltpu.make_async_copy(key_hbm, pairs_rows.at[pl.ds(0, key_width)], arrived.at[3]),
            pltpu.make_async_copy(
                value_hbm, pairs_rows.at[pl.ds(key_width, pair_width - key_width)], arrived.at[4]
            ),
        ] + [
            pltpu.make_async_copy(
                source, joined.at[:, pl.ds(start, source.shape[1])], arrived.at[i]
            )
            for i, (source, start) in enumerate(zip([query_hbm, in_hbm, gate_hbm], starts))
        ]
        gain_copy = pltpu.make_async_copy(gain_hbm, gain_ref, arrived.at[5])
        gain_copy.start()
        fetches[0].start()
        for copy in copies:
            copy.start()
        for fetch in fetches[1:]:
            fetch.start()

        def norm(i):
            widened = fetched[i].astype(jnp.float32)
            scale = lax.rsqrt(jnp.mean(widened * widened, axis=-1, keepdims=True) + NORM_EPSILON)
            normed[i] = (widened * scale * gain_ref[...]).astype(jnp.bfloat16)

        gain_copy.wait()
        fetches[0].wait()
        norm(0)
        for copy in copies[:2]:
            copy.wait()
        joined[:, heads_width : heads_width + pair_width] = pairs_rows[...].T
        for copy in copies[2:]:
            copy.wait()
        for i in range(blocks):
            if i + 1 < blocks:
                fetches[i + 1].wait()
            here = pl.ds(i * block, block)
            result = jnp.dot(normed[i], joined[...], preferred_element_type=jnp.float32)
            if i + 1 < blocks:
                norm(i + 1)
            queries_ref[here] = result[:, :heads_width].astype(jnp.bfloat16)
            pairs = result[:, heads_width : heads_width + pair_width].astype(jnp.bfloat16)
            pairs_ref[here] = pairs
            conv_in = result[:, starts[1] : starts[2]]
            conv_gate = result[:, starts[2] :]
            gated = (conv_in * jax.nn.sigmoid(conv_gate)).astype(jnp.bfloat16)
            gated_ref[here] = gated
            if i + 1 == blocks:
                tail_ref[:WINDOW] = pairs[block - WINDOW :]
                tail_ref[WINDOW:] = gated[block - HALO :]

    vmem = pl.BlockSpec(memory_space=pltpu.VMEM)
    in_hbm = [
        pltpu.with_memory_space_constraint(operand, pltpu.HBM)
        for operand in (
            norm_gain[None], tokens, query_weight, key_weight.T, value_weight.T, in_weight, gate_weight
        )
    ]
    return pl.pallas_call(
        body,
        in_specs=[pl.BlockSpec(memory_space=pl.ANY)] * 7,
        out_specs=[vmem] * 4,
        out_shape=[
            jax.ShapeDtypeStruct((rows, heads_width), jnp.bfloat16),
            jax.ShapeDtypeStruct((rows, pair_width), jnp.bfloat16),
            jax.ShapeDtypeStruct((rows, channels), jnp.bfloat16),
            jax.ShapeDtypeStruct((tail, channels), jnp.bfloat16),
        ],
        scratch_shapes=[
            pltpu.VMEM((blocks, block, width), jnp.bfloat16),
            pltpu.VMEM((blocks, block, width), jnp.bfloat16),
            pltpu.VMEM((width, heads_width + pair_width + 2 * channels), jnp.bfloat16),
            pltpu.VMEM((pair_width, width), jnp.bfloat16),
            pltpu.VMEM((1, width), jnp.float32),
            pltpu.SemaphoreType.DMA((6,)),
            pltpu.SemaphoreType.DMA((blocks,)),
        ],
        compiler_params=pltpu.CompilerParams(vmem_limit_bytes=24 << 20),
        name="project_inputs",
    )(*in_hbm)


def mix_rows(queries, pairs, gated, earlier, sinks, taps, shares):
    rows, heads_width = queries.shape
    channels = gated.shape[1]
    head_count = heads_width // HEAD_DIM
    share_rows = rows // shares

    def body(
        sinks_ref, queries_ref, pairs_ref, gated_ref, earlier_ref, taps_ref,
        out_ref, band, extended,
    ):
        band[:WINDOW] = earlier_ref[:WINDOW]
        band[WINDOW:] = pairs_ref[...]
        extended[:HALO] = earlier_ref[WINDOW:].astype(jnp.float32)
        extended[HALO:] = gated_ref[...].astype(jnp.float32)
        query_index = lax.broadcasted_iota(jnp.int32, (WINDOW, 2 * WINDOW), 0)
        key_index = lax.broadcasted_iota(jnp.int32, (WINDOW, 2 * WINDOW), 1)
        distance = WINDOW + query_index - key_index
        in_window = (distance >= 0) & (distance < WINDOW)
        not_before = in_window & ((lax.axis_index("sp") > 0) | (key_index >= WINDOW))
        own = pl.multiple_of(lax.axis_index("tp") * channels, channels)
        tap_rows = taps_ref[:, pl.ds(own, channels)].astype(jnp.float32)
        for block in range(rows // WINDOW):
            start = block * WINDOW
            share, inner = start // share_rows, start % share_rows
            keys = band[start : start + 2 * WINDOW, :HEAD_DIM]
            values = band[start : start + 2 * WINDOW, HEAD_DIM : 2 * HEAD_DIM]
            allowed = not_before if block == 0 else in_window
            found = []
            for head in range(head_count):
                here = queries_ref[start : start + WINDOW, head * HEAD_DIM : (head + 1) * HEAD_DIM]
                scores = lax.dot_general(
                    here, keys, (((1,), (1,)), ((), ())), preferred_element_type=jnp.float32
                ) * HEAD_DIM ** (-0.5)
                scores = jnp.where(allowed, scores, MASKED_SCORE)
                sink = sinks_ref[head]
                peak = jnp.maximum(jnp.max(scores, axis=-1, keepdims=True), sink)
                raised = jnp.exp(scores - peak)
                denominator = jnp.sum(raised, axis=-1, keepdims=True) + jnp.exp(sink - peak)
                weights = (raised * (1.0 / denominator)).astype(jnp.bfloat16)
                found.append(
                    jnp.dot(weights, values, preferred_element_type=jnp.float32).astype(jnp.bfloat16)
                )
            out_ref[share, inner : inner + WINDOW, :heads_width] = jnp.concatenate(found, axis=1)
            total = jnp.zeros((WINDOW, channels), jnp.float32)
            for tap in range(CONV_WIDTH):
                from_row = start + HALO - (CONV_WIDTH - 1) + tap
                total = total + tap_rows[tap : tap + 1] * extended[from_row : from_row + WINDOW]
            out_ref[share, inner : inner + WINDOW, heads_width:] = total.astype(jnp.bfloat16)

    whole = pl.BlockSpec(memory_space=pltpu.VMEM)
    scalars = pl.BlockSpec(memory_space=pltpu.SMEM)
    return pl.pallas_call(
        body,
        in_specs=[scalars] + [whole] * 5,
        out_specs=whole,
        out_shape=jax.ShapeDtypeStruct((shares, share_rows, heads_width + channels), jnp.bfloat16),
        scratch_shapes=[
            pltpu.VMEM((WINDOW + rows, pairs.shape[1]), jnp.bfloat16),
            pltpu.VMEM((HALO + rows, channels), jnp.float32),
        ],
        compiler_params=pltpu.CompilerParams(vmem_limit_bytes=12 << 20),
        name="mix_rows",
    )(sinks, queries, pairs, gated, earlier, taps)


def merge_mixers(exchanged, conv_gain, point_weight, output_gain):
    shares, rows, joint = exchanged.shape
    heads_width = joint // 2
    width = shares * heads_width

    def body(exchanged_ref, conv_gain_ref, point_ref, gain_ref, out_ref):
        attended = jnp.concatenate(
            [exchanged_ref[i, :, :heads_width] for i in range(shares)], axis=1
        ).astype(jnp.float32)
        convolved = jnp.concatenate(
            [exchanged_ref[i, :, heads_width:] for i in range(shares)], axis=1
        ).astype(jnp.float32)
        centered = convolved - jnp.mean(convolved, axis=-1, keepdims=True)
        scaled = (
            centered
            * lax.rsqrt(jnp.mean(centered * centered, axis=-1, keepdims=True) + NORM_EPSILON)
            * conv_gain_ref[...]
        )
        activated = (scaled * jax.nn.sigmoid(scaled)).astype(jnp.bfloat16)
        pointwise = jnp.dot(activated, point_ref[...], preferred_element_type=jnp.float32)
        out_ref[:, :width] = (
            attended
            * lax.rsqrt(jnp.mean(attended * attended, axis=-1, keepdims=True) + NORM_EPSILON)
            * gain_ref[:, :width]
        ).astype(jnp.bfloat16)
        out_ref[:, width:] = (
            pointwise
            * lax.rsqrt(jnp.mean(pointwise * pointwise, axis=-1, keepdims=True) + NORM_EPSILON)
            * gain_ref[:, width:]
        ).astype(jnp.bfloat16)

    return pl.pallas_call(
        body,
        out_shape=jax.ShapeDtypeStruct((rows, output_gain.shape[0]), jnp.bfloat16),
        compiler_params=pltpu.CompilerParams(vmem_limit_bytes=12 << 20),
        name="merge_mixers",
    )(exchanged, conv_gain[None], point_weight, output_gain[None])


def gather_shares(share, lines, tp_size):
    def number(line, side, lane):
        return (line * 2 + side) * tp_size + lane

    def send(block, target):
        found = []
        for line in range(lines):
            for side in range(2):
                for lane in range(tp_size):
                    to_line, to_side, to_lane = target(line, side, lane)
                    if 0 <= to_line < lines:
                        found.append((number(line, side, lane), number(to_line, to_side, to_lane)))
        return lax.ppermute(block, PLACE, found)

    def beside(line, side, lane):
        return (line + 1 if lane % 2 == 0 else line - 1), side, lane

    def beyond(line, side, lane):
        targets = far_lines(line, lines)
        if lane % 2 >= len(targets):
            return -1, side, lane
        to_line = targets[lane % 2]
        return to_line, side, lane - lane % 2 + far_lines(to_line, lines).index(line)

    def across(line, side, lane):
        return line, 1 - side, lane

    def lanes(line, side, lane):
        return line, side, lane ^ 1

    near = send(share, beside)
    far = send(share, beyond)
    half_rows = share.shape[0] // 2
    half = lax.dynamic_slice_in_dim(share, lax.axis_index("tp") % 2 * half_rows, half_rows, axis=0)
    traded = send(jnp.concatenate([near, half], axis=0), across)
    far_across = send(far, across)
    near_here = jnp.concatenate([near, traded], axis=0)
    near_there = send(near_here, lanes)
    far_there = send(far, lanes)
    far_across_there = send(far_across, lanes)
    return near_here, near_there, (far, far_there, far_across, far_across_there)


def far_lines(line, lines):
    return [other for other in range(lines) if abs(other - line) > 1]


def place_of_device():
    position, lane = lax.axis_index("sp"), lax.axis_index("tp") % 2
    return position // 2, position % 2, lane


def columns_of(merged_ref, from_line, sides, share_rows):
    found = []
    for at_side in sides:
        start = pl.multiple_of((from_line * 2 + at_side) * share_rows, share_rows)
        found.append(merged_ref[:, pl.ds(start, share_rows)])
    return jnp.concatenate(found, axis=1)


def near_product(merged, share, near_here, near_there, lines):
    rows, _ = merged.shape
    share_rows, columns = share.shape
    half_rows = share_rows // 2

    def body(merged_ref, share_ref, here_ref, there_ref, out_ref, pair):
        line, side, lane = place_of_device()

        def product(from_line, left):
            return jnp.dot(
                columns_of(merged_ref, from_line, (side, 1 - side), share_rows),
                left,
                preferred_element_type=jnp.float32,
            )

        pair[:share_rows] = share_ref[...]
        for ref, at_lane in ((here_ref, lane), (there_ref, 1 - lane)):
            start = pl.multiple_of(share_rows + at_lane * half_rows, half_rows)
            pair[pl.ds(start, half_rows)] = ref[2 * share_rows :]
        out_ref[...] = product(line, pair[...])

        for ref, at_lane in ((here_ref, lane), (there_ref, 1 - lane)):
            from_line = line - 1 + 2 * at_lane

            @pl.when((from_line >= 0) & (from_line < lines))
            def _():
                out_ref[...] += product(from_line, ref[: 2 * share_rows])

    vmem = pl.BlockSpec(memory_space=pltpu.VMEM)
    return pl.pallas_call(
        body,
        in_specs=[vmem] * 4,
        out_specs=vmem,
        out_shape=jax.ShapeDtypeStruct((rows, columns), jnp.float32),
        scratch_shapes=[pltpu.VMEM((2 * share_rows, columns), jnp.bfloat16)],
        compiler_params=pltpu.CompilerParams(vmem_limit_bytes=16 << 20),
        name="near_product",
    )(merged, share, near_here, near_there)


def far_product(merged, near_sum, far_pieces, lines):
    rows, _ = merged.shape
    share_rows, columns = far_pieces[0].shape
    chunk = 512

    def body(merged_ref, near_ref, *refs):
        piece_refs, out_hbm, rounded, sent = refs[:4], refs[4], refs[5], refs[6]
        line, side, lane = place_of_device()
        before = jnp.maximum(line - 1, 0)

        def other_line(index):
            found = jnp.where(index < before, index, line + 2 + index - before)
            return jnp.where(found < lines, found, -1)

        sources = [other_line(lane), other_line(1 - lane)]

        def finish(slots):
            left = [
                columns_of(merged_ref, sources[slot], (side, 1 - side), share_rows)
                for slot in slots
            ]
            left = jnp.concatenate(left, axis=1) if left else None
            copies = []
            for first in range(0, columns, chunk):
                here = slice(first, first + chunk)
                total = near_ref[:, here]
                if slots:
                    right = [piece_refs[2 * i + slot][:, here] for slot in slots for i in range(2)]
                    total = total + jnp.dot(
                        left, jnp.concatenate(right, axis=0), preferred_element_type=jnp.float32
                    )
                rounded[:, here] = total.astype(rounded.dtype)
                copies.append(
                    pltpu.make_async_copy(
                        rounded.at[:, pl.ds(first, chunk)],
                        out_hbm.at[:, pl.ds(first, chunk)],
                        sent.at[first // chunk],
                    )
                )
                copies[-1].start()
            for copy in copies:
                copy.wait()

        for slots in ((0, 1), (0,), (1,), ()):
            wanted = [(sources[slot] >= 0) == (slot in slots) for slot in range(2)]

            @pl.when(wanted[0] & wanted[1])
            def _():
                finish(slots)

    vmem = pl.BlockSpec(memory_space=pltpu.VMEM)
    return pl.pallas_call(
        body,
        in_specs=[vmem] * 6,
        out_specs=pl.BlockSpec(memory_space=pl.ANY),
        out_shape=pltpu.HBM((rows, columns), jnp.bfloat16),
        scratch_shapes=[
            pltpu.VMEM((rows, columns), jnp.bfloat16),
            pltpu.SemaphoreType.DMA((columns // chunk,)),
        ],
        compiler_params=pltpu.CompilerParams(vmem_limit_bytes=16 << 20),
        name="far_product",
    )(merged, near_sum, *far_pieces)


def on_device(
    tokens,
    norm_gain,
    query_weight,
    key_weight,
    value_weight,
    sink_logits,
    conv_in_weight,
    conv_gate_weight,
    conv_taps,
    conv_gain,
    point_weight,
    output_gain,
    output_weight,
):
    sp_size, tp_size = lax.axis_size("sp"), lax.axis_size("tp")
    lines = sp_size // 2
    by_shares = sends_shares(sp_size, tp_size)
    if by_shares:
        near_here, near_there, far_pieces = gather_shares(output_weight, lines, tp_size)
    queries, pairs, gated, tail = project_inputs(
        tokens, norm_gain, query_weight, key_weight, value_weight, conv_in_weight, conv_gate_weight
    )
    earlier = from_behind(tail, "sp", 1)
    mixed = mix_rows(queries, pairs, gated, earlier, sink_logits, conv_taps, tp_size)
    exchanged = lax.all_to_all(mixed, "tp", split_axis=0, concat_axis=0, tiled=True)
    merged = merge_mixers(exchanged, conv_gain, point_weight, output_gain)
    if by_shares:
        near_sum = near_product(merged, output_weight, near_here, near_there, lines)
        return far_product(merged, near_sum, far_pieces, lines)
    projected = jnp.dot(
        merged,
        lax.all_gather(output_weight, "sp", axis=0, tiled=True),
        preferred_element_type=jnp.float32,
    )
    return projected.astype(jnp.bfloat16)


def sends_shares(sp_size, tp_size):
    return sp_size % 2 == 0 and tp_size % 2 == 0 and 3 <= sp_size // 2 <= 4


def solution(mesh):
    in_specs = (
        P("sp", None),
        P(),
        P(None, "tp"),
        P(None, "tp"),
        P(None, "tp"),
        P("tp"),
        P(None, "tp"),
        P(None, "tp"),
        P(),
        P(),
        P(),
        P(),
        P("sp", None),
    )
    out_specs = P(("sp", "tp"), None)
    return jax.shard_map(
        on_device, mesh=mesh, in_specs=in_specs, out_specs=out_specs, check_vma=False
    )
```

```python
import jax
import jax.numpy as jnp
from jax import lax
from jax.experimental import pallas as pl
from jax.experimental.pallas import tpu as pltpu
from jax.sharding import PartitionSpec as P


HEAD_DIM = 64
WINDOW = 128
CONV_WIDTH = 31


NORM_EPSILON = 1e-06
MASKED_SCORE = -1e30
HALO = 32


PLACE = ("sp", "tp")


def from_behind(block, axis, distance):
    devices = range(lax.axis_size(axis))
    route = [(i - distance, i) for i in devices if i - distance in devices]
    return lax.ppermute(block, axis, route)


def project_inputs(tokens, norm_gain, query_weight, key_weight, value_weight, in_weight, gate_weight):
    rows, width = tokens.shape
    heads_width, pair_width = query_weight.shape[1], key_weight.shape[1] + value_weight.shape[1]
    key_width, channels = key_weight.shape[1], in_weight.shape[1]
    block = 256
    blocks = rows // block
    tail = WINDOW + HALO
    starts = [0, heads_width + pair_width, heads_width + pair_width + channels]

    def body(
        gain_hbm, tokens_hbm, query_hbm, key_hbm, value_hbm, in_hbm, gate_hbm,
        queries_ref, pairs_ref, gated_ref, tail_ref,
        fetched, normed, joined, pairs_rows, gain_ref, arrived, fetched_sem,
    ):
        fetches = [
            pltpu.make_async_copy(
                tokens_hbm.at[pl.ds(i * block, block)], fetched.at[i], fetched_sem.at[i]
            )
            for i in range(blocks)
        ]
        copies = [
            pltpu.make_async_copy(key_hbm, pairs_rows.at[pl.ds(0, key_width)], arrived.at[3]),
            pltpu.make_async_copy(
                value_hbm, pairs_rows.at[pl.ds(key_width, pair_width - key_width)], arrived.at[4]
            ),
        ] + [
            pltpu.make_async_copy(
                source, joined.at[:, pl.ds(start, source.shape[1])], arrived.at[i]
            )
            for i, (source, start) in enumerate(zip([query_hbm, in_hbm, gate_hbm], starts))
        ]
        gain_copy = pltpu.make_async_copy(gain_hbm, gain_ref, arrived.at[5])
        gain_copy.start()
        fetches[0].start()
        for copy in copies:
            copy.start()
        for fetch in fetches[1:]:
            fetch.start()

        def norm(i):
            widened = fetched[i].astype(jnp.float32)
            scale = lax.rsqrt(jnp.mean(widened * widened, axis=-1, keepdims=True) + NORM_EPSILON)
            normed[i] = (widened * scale * gain_ref[...]).astype(jnp.bfloat16)

        gain_copy.wait()
        fetches[0].wait()
        norm(0)
        for copy in copies[:2]:
            copy.wait()
        joined[:, heads_width : heads_width + pair_width] = pairs_rows[...].T
        for copy in copies[2:]:
            copy.wait()
        for i in range(blocks):
            if i + 1 < blocks:
                fetches[i + 1].wait()
            here = pl.ds(i * block, block)
            result = jnp.dot(normed[i], joined[...], preferred_element_type=jnp.float32)
            if i + 1 < blocks:
                norm(i + 1)
            queries_ref[here] = result[:, :heads_width].astype(jnp.bfloat16)
            pairs = result[:, heads_width : heads_width + pair_width].astype(jnp.bfloat16)
            pairs_ref[here] = pairs
            conv_in = result[:, starts[1] : starts[2]]
            conv_gate = result[:, starts[2] :]
            gated = (conv_in * jax.nn.sigmoid(conv_gate)).astype(jnp.bfloat16)
            gated_ref[here] = gated
            if i + 1 == blocks:
                tail_ref[:WINDOW] = pairs[block - WINDOW :]
                tail_ref[WINDOW:] = gated[block - HALO :]

    vmem = pl.BlockSpec(memory_space=pltpu.VMEM)
    in_hbm = [
        pltpu.with_memory_space_constraint(operand, pltpu.HBM)
        for operand in (
            norm_gain[None], tokens, query_weight, key_weight.T, value_weight.T, in_weight, gate_weight
        )
    ]
    return pl.pallas_call(
        body,
        in_specs=[pl.BlockSpec(memory_space=pl.ANY)] * 7,
        out_specs=[vmem] * 4,
        out_shape=[
            jax.ShapeDtypeStruct((rows, heads_width), jnp.bfloat16),
            jax.ShapeDtypeStruct((rows, pair_width), jnp.bfloat16),
            jax.ShapeDtypeStruct((rows, channels), jnp.bfloat16),
            jax.ShapeDtypeStruct((tail, channels), jnp.bfloat16),
        ],
        scratch_shapes=[
            pltpu.VMEM((blocks, block, width), jnp.bfloat16),
            pltpu.VMEM((blocks, block, width), jnp.bfloat16),
            pltpu.VMEM((width, heads_width + pair_width + 2 * channels), jnp.bfloat16),
            pltpu.VMEM((pair_width, width), jnp.bfloat16),
            pltpu.VMEM((1, width), jnp.float32),
            pltpu.SemaphoreType.DMA((6,)),
            pltpu.SemaphoreType.DMA((blocks,)),
        ],
        compiler_params=pltpu.CompilerParams(vmem_limit_bytes=24 << 20),
        name="project_inputs",
    )(*in_hbm)


def mix_rows(queries, pairs, gated, earlier, sinks, taps, shares):
    rows, heads_width = queries.shape
    channels = gated.shape[1]
    head_count = heads_width // HEAD_DIM
    share_rows = rows // shares

    def body(
        sinks_ref, queries_ref, pairs_ref, gated_ref, earlier_ref, taps_ref,
        out_ref, band, extended,
    ):
        band[:WINDOW] = earlier_ref[:WINDOW]
        band[WINDOW:] = pairs_ref[...]
        extended[:HALO] = earlier_ref[WINDOW:].astype(jnp.float32)
        extended[HALO:] = gated_ref[...].astype(jnp.float32)
        query_index = lax.broadcasted_iota(jnp.int32, (WINDOW, 2 * WINDOW), 0)
        key_index = lax.broadcasted_iota(jnp.int32, (WINDOW, 2 * WINDOW), 1)
        distance = WINDOW + query_index - key_index
        in_window = (distance >= 0) & (distance < WINDOW)
        not_before = in_window & ((lax.axis_index("sp") > 0) | (key_index >= WINDOW))
        own = pl.multiple_of(lax.axis_index("tp") * channels, channels)
        tap_rows = taps_ref[:, pl.ds(own, channels)].astype(jnp.float32)
        for block in range(rows // WINDOW):
            start = block * WINDOW
            share, inner = start // share_rows, start % share_rows
            keys = band[start : start + 2 * WINDOW, :HEAD_DIM]
            values = band[start : start + 2 * WINDOW, HEAD_DIM : 2 * HEAD_DIM]
            allowed = not_before if block == 0 else in_window
            found = []
            for head in range(head_count):
                here = queries_ref[start : start + WINDOW, head * HEAD_DIM : (head + 1) * HEAD_DIM]
                scores = lax.dot_general(
                    here, keys, (((1,), (1,)), ((), ())), preferred_element_type=jnp.float32
                ) * HEAD_DIM ** (-0.5)
                scores = jnp.where(allowed, scores, MASKED_SCORE)
                sink = sinks_ref[head]
                peak = jnp.maximum(jnp.max(scores, axis=-1, keepdims=True), sink)
                raised = jnp.exp(scores - peak)
                denominator = jnp.sum(raised, axis=-1, keepdims=True) + jnp.exp(sink - peak)
                weights = (raised * (1.0 / denominator)).astype(jnp.bfloat16)
                found.append(
                    jnp.dot(weights, values, preferred_element_type=jnp.float32).astype(jnp.bfloat16)
                )
            out_ref[share, inner : inner + WINDOW, :heads_width] = jnp.concatenate(found, axis=1)
            total = jnp.zeros((WINDOW, channels), jnp.float32)
            for tap in range(CONV_WIDTH):
                from_row = start + HALO - (CONV_WIDTH - 1) + tap
                total = total + tap_rows[tap : tap + 1] * extended[from_row : from_row + WINDOW]
            out_ref[share, inner : inner + WINDOW, heads_width:] = total.astype(jnp.bfloat16)

    whole = pl.BlockSpec(memory_space=pltpu.VMEM)
    scalars = pl.BlockSpec(memory_space=pltpu.SMEM)
    return pl.pallas_call(
        body,
        in_specs=[scalars] + [whole] * 5,
        out_specs=whole,
        out_shape=jax.ShapeDtypeStruct((shares, share_rows, heads_width + channels), jnp.bfloat16),
        scratch_shapes=[
            pltpu.VMEM((WINDOW + rows, pairs.shape[1]), jnp.bfloat16),
            pltpu.VMEM((HALO + rows, channels), jnp.float32),
        ],
        compiler_params=pltpu.CompilerParams(vmem_limit_bytes=12 << 20),
        name="mix_rows",
    )(sinks, queries, pairs, gated, earlier, taps)


def merge_mixers(exchanged, conv_gain, point_weight, output_gain):
    shares, rows, joint = exchanged.shape
    heads_width = joint // 2
    width = shares * heads_width

    def body(exchanged_ref, conv_gain_ref, point_ref, gain_ref, out_ref):
        attended = jnp.concatenate(
            [exchanged_ref[i, :, :heads_width] for i in range(shares)], axis=1
        ).astype(jnp.float32)
        convolved = jnp.concatenate(
            [exchanged_ref[i, :, heads_width:] for i in range(shares)], axis=1
        ).astype(jnp.float32)
        centered = convolved - jnp.mean(convolved, axis=-1, keepdims=True)
        scaled = (
            centered
            * lax.rsqrt(jnp.mean(centered * centered, axis=-1, keepdims=True) + NORM_EPSILON)
            * conv_gain_ref[...]
        )
        activated = (scaled * jax.nn.sigmoid(scaled)).astype(jnp.bfloat16)
        pointwise = jnp.dot(activated, point_ref[...], preferred_element_type=jnp.float32)
        out_ref[:, :width] = (
            attended
            * lax.rsqrt(jnp.mean(attended * attended, axis=-1, keepdims=True) + NORM_EPSILON)
            * gain_ref[:, :width]
        ).astype(jnp.bfloat16)
        out_ref[:, width:] = (
            pointwise
            * lax.rsqrt(jnp.mean(pointwise * pointwise, axis=-1, keepdims=True) + NORM_EPSILON)
            * gain_ref[:, width:]
        ).astype(jnp.bfloat16)

    return pl.pallas_call(
        body,
        out_shape=jax.ShapeDtypeStruct((rows, output_gain.shape[0]), jnp.bfloat16),
        compiler_params=pltpu.CompilerParams(vmem_limit_bytes=12 << 20),
        name="merge_mixers",
    )(exchanged, conv_gain[None], point_weight, output_gain[None])


def gather_shares(share, lines, tp_size):
    def number(line, side, lane):
        return (line * 2 + side) * tp_size + lane

    def send(block, target):
        found = []
        for line in range(lines):
            for side in range(2):
                for lane in range(tp_size):
                    to_line, to_side, to_lane = target(line, side, lane)
                    if 0 <= to_line < lines:
                        found.append((number(line, side, lane), number(to_line, to_side, to_lane)))
        return lax.ppermute(block, PLACE, found)

    def beside(line, side, lane):
        return (line + 1 if lane % 2 == 0 else line - 1), side, lane

    def beyond(line, side, lane):
        targets = far_lines(line, lines)
        if lane % 2 >= len(targets):
            return -1, side, lane
        to_line = targets[lane % 2]
        to_side = 1 - side if lane // 2 % 2 else side
        return to_line, to_side, lane - lane % 2 + far_lines(to_line, lines).index(line)

    def lower_lane_across(line, side, lane):
        return (line if lane % 2 == 0 else -1), 1 - side, lane

    def holders_across(line, side, lane):
        from_line = line - 1 if lane % 2 == 0 else line + 1
        return (line if 0 <= from_line < lines else -1), 1 - side, lane

    def holders_to_neighbours(line, side, lane):
        held = lane % 2 < len(far_lines(line, lines))
        to = (1 - side, lane) if lane % 2 == 0 else (side, lane ^ 2)
        return (line if held else -1), *to

    def lanes(line, side, lane):
        return line, side, lane ^ 1

    near = send(share, beside)
    opposite = send(share, lower_lane_across)
    near_across = send(near, holders_across)
    far = send(share, beyond)
    far_other = send(far, holders_to_neighbours)
    near_here = jnp.concatenate([near, near_across, opposite], axis=0)
    near_there = send(near_here, lanes)
    far_there = send(far, lanes)
    far_other_there = send(far_other, lanes)
    return near_here, near_there, (far, far_there, far_other, far_other_there)


def far_lines(line, lines):
    return [other for other in range(lines) if abs(other - line) > 1]


def place_of_device():
    position, lane = lax.axis_index("sp"), lax.axis_index("tp") % 2
    return position // 2, position % 2, lane


def columns_of(merged_ref, from_line, sides, share_rows):
    found = []
    for at_side in sides:
        start = pl.multiple_of((from_line * 2 + at_side) * share_rows, share_rows)
        found.append(merged_ref[:, pl.ds(start, share_rows)])
    return jnp.concatenate(found, axis=1)


def near_product(merged, share, near_here, near_there, lines):
    rows, _ = merged.shape
    share_rows, columns = share.shape

    def body(merged_ref, share_ref, here_ref, there_ref, out_ref):
        line, side, lane = place_of_device()

        def product(from_line, left):
            return jnp.dot(
                columns_of(merged_ref, from_line, (side, 1 - side), share_rows),
                left,
                preferred_element_type=jnp.float32,
            )

        for ref, holds in ((here_ref, lane == 0), (there_ref, lane == 1)):

            @pl.when(holds)
            def _():
                pair = jnp.concatenate([share_ref[...], ref[2 * share_rows :]], axis=0)
                out_ref[...] = product(line, pair)

        for ref, at_lane in ((here_ref, lane), (there_ref, 1 - lane)):
            from_line = line - 1 + 2 * at_lane

            @pl.when((from_line >= 0) & (from_line < lines))
            def _():
                out_ref[...] += product(from_line, ref[: 2 * share_rows])

    vmem = pl.BlockSpec(memory_space=pltpu.VMEM)
    return pl.pallas_call(
        body,
        in_specs=[vmem] * 4,
        out_specs=vmem,
        out_shape=jax.ShapeDtypeStruct((rows, columns), jnp.float32),
        compiler_params=pltpu.CompilerParams(vmem_limit_bytes=16 << 20),
        name="near_product",
    )(merged, share, near_here, near_there)


def far_product(merged, near_sum, far_pieces, lines):
    rows, _ = merged.shape
    share_rows, columns = far_pieces[0].shape
    chunk = 512

    def body(merged_ref, near_ref, *refs):
        piece_refs, out_hbm, rounded, sent = refs[:4], refs[4], refs[5], refs[6]
        line, side, lane = place_of_device()
        first_side = jnp.where(lax.axis_index("tp") // 2 % 2 == 1, 1 - side, side)
        before = jnp.maximum(line - 1, 0)

        def other_line(index):
            found = jnp.where(index < before, index, line + 2 + index - before)
            return jnp.where(found < lines, found, -1)

        sources = [other_line(lane), other_line(1 - lane)]

        def finish(slots):
            left = [
                columns_of(merged_ref, sources[slot], (first_side, 1 - first_side), share_rows)
                for slot in slots
            ]
            left = jnp.concatenate(left, axis=1) if left else None
            copies = []
            for first in range(0, columns, chunk):
                here = slice(first, first + chunk)
                total = near_ref[:, here]
                if slots:
                    right = [piece_refs[2 * i + slot][:, here] for slot in slots for i in range(2)]
                    total = total + jnp.dot(
                        left, jnp.concatenate(right, axis=0), preferred_element_type=jnp.float32
                    )
                rounded[:, here] = total.astype(rounded.dtype)
                copies.append(
                    pltpu.make_async_copy(
                        rounded.at[:, pl.ds(first, chunk)],
                        out_hbm.at[:, pl.ds(first, chunk)],
                        sent.at[first // chunk],
                    )
                )
                copies[-1].start()
            for copy in copies:
                copy.wait()

        for slots in ((0, 1), (0,), (1,), ()):
            wanted = [(sources[slot] >= 0) == (slot in slots) for slot in range(2)]

            @pl.when(wanted[0] & wanted[1])
            def _():
                finish(slots)

    vmem = pl.BlockSpec(memory_space=pltpu.VMEM)
    return pl.pallas_call(
        body,
        in_specs=[vmem] * 6,
        out_specs=pl.BlockSpec(memory_space=pl.ANY),
        out_shape=pltpu.HBM((rows, columns), jnp.bfloat16),
        scratch_shapes=[
            pltpu.VMEM((rows, columns), jnp.bfloat16),
            pltpu.SemaphoreType.DMA((columns // chunk,)),
        ],
        compiler_params=pltpu.CompilerParams(vmem_limit_bytes=16 << 20),
        name="far_product",
    )(merged, near_sum, *far_pieces)


def on_device(
    tokens,
    norm_gain,
    query_weight,
    key_weight,
    value_weight,
    sink_logits,
    conv_in_weight,
    conv_gate_weight,
    conv_taps,
    conv_gain,
    point_weight,
    output_gain,
    output_weight,
):
    sp_size, tp_size = lax.axis_size("sp"), lax.axis_size("tp")
    lines = sp_size // 2
    by_shares = sends_shares(sp_size, tp_size)
    if by_shares:
        near_here, near_there, far_pieces = gather_shares(output_weight, lines, tp_size)
    queries, pairs, gated, tail = project_inputs(
        tokens, norm_gain, query_weight, key_weight, value_weight, conv_in_weight, conv_gate_weight
    )
    earlier = from_behind(tail, "sp", 1)
    mixed = mix_rows(queries, pairs, gated, earlier, sink_logits, conv_taps, tp_size)
    exchanged = lax.all_to_all(mixed, "tp", split_axis=0, concat_axis=0, tiled=True)
    merged = merge_mixers(exchanged, conv_gain, point_weight, output_gain)
    if by_shares:
        near_sum = near_product(merged, output_weight, near_here, near_there, lines)
        return far_product(merged, near_sum, far_pieces, lines)
    projected = jnp.dot(
        merged,
        lax.all_gather(output_weight, "sp", axis=0, tiled=True),
        preferred_element_type=jnp.float32,
    )
    return projected.astype(jnp.bfloat16)


def sends_shares(sp_size, tp_size):
    return sp_size % 2 == 0 and tp_size % 4 == 0 and 3 <= sp_size // 2 <= 4


def solution(mesh):
    in_specs = (
        P("sp", None),
        P(),
        P(None, "tp"),
        P(None, "tp"),
        P(None, "tp"),
        P("tp"),
        P(None, "tp"),
        P(None, "tp"),
        P(),
        P(),
        P(),
        P(),
        P("sp", None),
    )
    out_specs = P(("sp", "tp"), None)
    return jax.shard_map(
        on_device, mesh=mesh, in_specs=in_specs, out_specs=out_specs, check_vma=False
    )
```

```python
import jax
import jax.numpy as jnp
from jax import lax
from jax.experimental import pallas as pl
from jax.experimental.pallas import tpu as pltpu
from jax.sharding import PartitionSpec as P


HEAD_DIM = 64
WINDOW = 128
CONV_WIDTH = 31


NORM_EPSILON = 1e-06
MASKED_SCORE = -1e30
HALO = 32


PLACE = ("sp", "tp")


def from_behind(block, axis, distance):
    devices = range(lax.axis_size(axis))
    route = [(i - distance, i) for i in devices if i - distance in devices]
    return lax.ppermute(block, axis, route)


BLOCK = 256


def normed_rows(token_rows, gain):
    widened = token_rows.astype(jnp.float32)
    scale = lax.rsqrt(jnp.mean(widened * widened, axis=-1, keepdims=True) + NORM_EPSILON)
    return (widened * scale * gain).astype(jnp.bfloat16)


def split_product(normed, joined, heads_width, pair_width, channels):
    result = jnp.dot(normed, joined, preferred_element_type=jnp.float32)
    pairs_end = heads_width + pair_width
    conv_in = result[:, pairs_end : pairs_end + channels]
    gated = conv_in * jax.nn.sigmoid(result[:, pairs_end + channels :])
    return [
        part.astype(jnp.bfloat16)
        for part in (result[:, :heads_width], result[:, heads_width:pairs_end], gated)
    ]


def project_last(tokens, norm_gain, query_weight, key_weight, value_weight, in_weight, gate_weight):
    rows, width = tokens.shape
    heads_width, key_width, channels = query_weight.shape[1], key_weight.shape[1], in_weight.shape[1]
    pair_width = key_width + value_weight.shape[1]
    tail = WINDOW + HALO
    others = rows - BLOCK
    starts = [0, heads_width + pair_width, heads_width + pair_width + channels]

    def body(
        gain_hbm, tokens_hbm, query_hbm, key_hbm, value_hbm, in_hbm, gate_hbm,
        queries_ref, pairs_ref, gated_ref, tail_ref, joined, rest_ref,
        last_ref, pairs_rows, gain_ref, arrived,
    ):
        copies = [
            pltpu.make_async_copy(source, target, arrived.at[i])
            for i, (source, target) in enumerate(
                [
                    (gain_hbm, gain_ref),
                    (tokens_hbm.at[pl.ds(others, BLOCK)], last_ref),
                    (key_hbm, pairs_rows.at[pl.ds(0, key_width)]),
                    (value_hbm, pairs_rows.at[pl.ds(key_width, pair_width - key_width)]),
                ]
                + [
                    (source, joined.at[:, pl.ds(start, source.shape[1])])
                    for source, start in zip([query_hbm, in_hbm, gate_hbm], starts)
                ]
                + [(tokens_hbm.at[pl.ds(0, others)], rest_ref)]
            )
        ]
        for copy in copies:
            copy.start()
        for copy in copies[:2]:
            copy.wait()
        normed = normed_rows(last_ref[...], gain_ref[...])
        for copy in copies[2:4]:
            copy.wait()
        joined[:, heads_width : heads_width + pair_width] = pairs_rows[...].T
        for copy in copies[4:7]:
            copy.wait()
        queries, pairs, gated = split_product(
            normed, joined[...], heads_width, pair_width, channels
        )
        queries_ref[...] = queries
        pairs_ref[...] = pairs
        gated_ref[...] = gated
        tail_ref[:WINDOW] = pairs[BLOCK - WINDOW :]
        tail_ref[WINDOW:] = gated[BLOCK - HALO :]
        copies[7].wait()

    vmem = pl.BlockSpec(memory_space=pltpu.VMEM)
    in_hbm = [
        pltpu.with_memory_space_constraint(operand, pltpu.HBM)
        for operand in (
            norm_gain[None], tokens, query_weight, key_weight.T, value_weight.T, in_weight,
            gate_weight,
        )
    ]
    shapes = [
        (BLOCK, heads_width), (BLOCK, pair_width), (BLOCK, channels), (tail, channels),
        (width, heads_width + pair_width + 2 * channels), (others, width),
    ]
    return pl.pallas_call(
        body,
        in_specs=[pl.BlockSpec(memory_space=pl.ANY)] * 7,
        out_specs=[vmem] * len(shapes),
        out_shape=[jax.ShapeDtypeStruct(shape, jnp.bfloat16) for shape in shapes],
        scratch_shapes=[
            pltpu.VMEM((BLOCK, width), jnp.bfloat16),
            pltpu.VMEM((pair_width, width), jnp.bfloat16),
            pltpu.VMEM((1, width), jnp.float32),
            pltpu.SemaphoreType.DMA((8,)),
        ],
        compiler_params=pltpu.CompilerParams(vmem_limit_bytes=20 << 20),
        name="project_last",
    )(*in_hbm)


def project_rest(tokens, norm_gain, joined, heads_width, pair_width):
    rows, width = tokens.shape
    channels = (joined.shape[1] - heads_width - pair_width) // 2
    blocks = rows // BLOCK

    def body(gain_ref, tokens_ref, joined_ref, queries_ref, pairs_ref, gated_ref, normed):
        normed[0] = normed_rows(tokens_ref[:BLOCK], gain_ref[...])
        for i in range(blocks):
            here = slice(i * BLOCK, (i + 1) * BLOCK)
            queries, pairs, gated = split_product(
                normed[i], joined_ref[...], heads_width, pair_width, channels
            )
            if i + 1 < blocks:
                following = tokens_ref[(i + 1) * BLOCK : (i + 2) * BLOCK]
                normed[i + 1] = normed_rows(following, gain_ref[...])
            queries_ref[here] = queries
            pairs_ref[here] = pairs
            gated_ref[here] = gated

    vmem = pl.BlockSpec(memory_space=pltpu.VMEM)
    return pl.pallas_call(
        body,
        in_specs=[vmem] * 3,
        out_specs=[vmem] * 3,
        out_shape=[
            jax.ShapeDtypeStruct((rows, columns), jnp.bfloat16)
            for columns in (heads_width, pair_width, channels)
        ],
        scratch_shapes=[pltpu.VMEM((blocks, BLOCK, width), jnp.bfloat16)],
        compiler_params=pltpu.CompilerParams(vmem_limit_bytes=24 << 20),
        name="project_rest",
    )(norm_gain[None], tokens, joined)


def mix_rows(first_rows, last_rows, earlier, sinks, taps, shares):
    rest, heads_width = first_rows[0].shape
    rows = rest + last_rows[0].shape[0]
    pair_width, channels = first_rows[1].shape[1], first_rows[2].shape[1]
    head_count = heads_width // HEAD_DIM
    share_rows = rows // shares

    def body(
        sinks_ref, queries_ref, pairs_ref, gated_ref, last_queries, last_pairs, last_gated,
        earlier_ref, taps_ref, out_ref, band, extended,
    ):
        band[:WINDOW] = earlier_ref[:WINDOW]
        band[WINDOW : WINDOW + rest] = pairs_ref[...]
        band[WINDOW + rest :] = last_pairs[...]
        extended[:HALO] = earlier_ref[WINDOW:].astype(jnp.float32)
        extended[HALO : HALO + rest] = gated_ref[...].astype(jnp.float32)
        extended[HALO + rest :] = last_gated[...].astype(jnp.float32)
        query_index = lax.broadcasted_iota(jnp.int32, (WINDOW, 2 * WINDOW), 0)
        key_index = lax.broadcasted_iota(jnp.int32, (WINDOW, 2 * WINDOW), 1)
        distance = WINDOW + query_index - key_index
        in_window = (distance >= 0) & (distance < WINDOW)
        not_before = in_window & ((lax.axis_index("sp") > 0) | (key_index >= WINDOW))
        own = pl.multiple_of(lax.axis_index("tp") * channels, channels)
        tap_rows = taps_ref[:, pl.ds(own, channels)].astype(jnp.float32)
        for block in range(rows // WINDOW):
            start = block * WINDOW
            share, inner = start // share_rows, start % share_rows
            keys = band[start : start + 2 * WINDOW, :HEAD_DIM]
            values = band[start : start + 2 * WINDOW, HEAD_DIM : 2 * HEAD_DIM]
            allowed = not_before if block == 0 else in_window
            found = []
            for head in range(head_count):
                source, at = (queries_ref, start) if start < rest else (last_queries, start - rest)
                here = source[at : at + WINDOW, head * HEAD_DIM : (head + 1) * HEAD_DIM]
                scores = lax.dot_general(
                    here, keys, (((1,), (1,)), ((), ())), preferred_element_type=jnp.float32
                ) * HEAD_DIM ** (-0.5)
                scores = jnp.where(allowed, scores, MASKED_SCORE)
                sink = sinks_ref[head]
                peak = jnp.maximum(jnp.max(scores, axis=-1, keepdims=True), sink)
                raised = jnp.exp(scores - peak)
                denominator = jnp.sum(raised, axis=-1, keepdims=True) + jnp.exp(sink - peak)
                weights = (raised * (1.0 / denominator)).astype(jnp.bfloat16)
                found.append(
                    jnp.dot(weights, values, preferred_element_type=jnp.float32).astype(jnp.bfloat16)
                )
            out_ref[share, inner : inner + WINDOW, :heads_width] = jnp.concatenate(found, axis=1)
            total = jnp.zeros((WINDOW, channels), jnp.float32)
            for tap in range(CONV_WIDTH):
                from_row = start + HALO - (CONV_WIDTH - 1) + tap
                total = total + tap_rows[tap : tap + 1] * extended[from_row : from_row + WINDOW]
            out_ref[share, inner : inner + WINDOW, heads_width:] = total.astype(jnp.bfloat16)

    whole = pl.BlockSpec(memory_space=pltpu.VMEM)
    scalars = pl.BlockSpec(memory_space=pltpu.SMEM)
    return pl.pallas_call(
        body,
        in_specs=[scalars] + [whole] * 8,
        out_specs=whole,
        out_shape=jax.ShapeDtypeStruct((shares, share_rows, heads_width + channels), jnp.bfloat16),
        scratch_shapes=[
            pltpu.VMEM((WINDOW + rows, pair_width), jnp.bfloat16),
            pltpu.VMEM((HALO + rows, channels), jnp.float32),
        ],
        compiler_params=pltpu.CompilerParams(vmem_limit_bytes=12 << 20),
        name="mix_rows",
    )(sinks, *first_rows, *last_rows, earlier, taps)


def merge_mixers(exchanged, conv_gain, point_weight, output_gain):
    shares, rows, joint = exchanged.shape
    heads_width = joint // 2
    width = shares * heads_width

    def body(exchanged_ref, conv_gain_ref, point_ref, gain_ref, out_ref):
        attended = jnp.concatenate(
            [exchanged_ref[i, :, :heads_width] for i in range(shares)], axis=1
        ).astype(jnp.float32)
        convolved = jnp.concatenate(
            [exchanged_ref[i, :, heads_width:] for i in range(shares)], axis=1
        ).astype(jnp.float32)
        centered = convolved - jnp.mean(convolved, axis=-1, keepdims=True)
        scaled = (
            centered
            * lax.rsqrt(jnp.mean(centered * centered, axis=-1, keepdims=True) + NORM_EPSILON)
            * conv_gain_ref[...]
        )
        activated = (scaled * jax.nn.sigmoid(scaled)).astype(jnp.bfloat16)
        pointwise = jnp.dot(activated, point_ref[...], preferred_element_type=jnp.float32)
        out_ref[:, :width] = (
            attended
            * lax.rsqrt(jnp.mean(attended * attended, axis=-1, keepdims=True) + NORM_EPSILON)
            * gain_ref[:, :width]
        ).astype(jnp.bfloat16)
        out_ref[:, width:] = (
            pointwise
            * lax.rsqrt(jnp.mean(pointwise * pointwise, axis=-1, keepdims=True) + NORM_EPSILON)
            * gain_ref[:, width:]
        ).astype(jnp.bfloat16)

    return pl.pallas_call(
        body,
        out_shape=jax.ShapeDtypeStruct((rows, output_gain.shape[0]), jnp.bfloat16),
        compiler_params=pltpu.CompilerParams(vmem_limit_bytes=12 << 20),
        name="merge_mixers",
    )(exchanged, conv_gain[None], point_weight, output_gain[None])


class ShareRoutes:
    def __init__(self, lines, tp_size):
        self.lines, self.tp_size = lines, tp_size

    def number(self, line, side, lane):
        return (line * 2 + side) * self.tp_size + lane

    def send(self, block, target):
        found = []
        for line in range(self.lines):
            for side in range(2):
                for lane in range(self.tp_size):
                    to = target(line, side, lane)
                    if 0 <= to[0] < self.lines:
                        found.append((self.number(line, side, lane), self.number(*to)))
        return lax.ppermute(block, PLACE, found)

    def beside(self, line, side, lane):
        return (line + 1 if lane % 2 == 0 else line - 1), side, lane

    def beyond(self, line, side, lane):
        targets = far_lines(line, self.lines)
        if lane % 2 >= len(targets):
            return -1, side, lane
        to_line = targets[lane % 2]
        to_side = 1 - side if lane // 2 % 2 else side
        to_lane = lane - lane % 2 + far_lines(to_line, self.lines).index(line)
        return to_line, to_side, to_lane

    def holders_across(self, line, side, lane):
        from_line = line - 1 if lane % 2 == 0 else line + 1
        return (line if 0 <= from_line < self.lines else -1), 1 - side, lane

    def lower_lane_across(self, line, side, lane):
        return (line if lane % 2 == 0 else -1), 1 - side, lane

    def upper_lane_from_lower(self, line, side, lane):
        return (line if lane % 2 == 0 else -1), side, lane ^ 1

    def to_neighbours(self, line, side, lane):
        held = lane % 2 < len(far_lines(line, self.lines))
        to = (1 - side, lane) if lane % 2 == 0 else (side, lane ^ 2)
        return (line if held else -1), *to

    def lanes(self, line, side, lane):
        return line, side, lane ^ 1


def far_lines(line, lines):
    return [other for other in range(lines) if abs(other - line) > 1]


def place_of_device():
    position, lane = lax.axis_index("sp"), lax.axis_index("tp") % 2
    return position // 2, position % 2, lane


def columns_of(merged_ref, from_line, sides, share_rows):
    found = []
    for at_side in sides:
        start = pl.multiple_of((from_line * 2 + at_side) * share_rows, share_rows)
        found.append(merged_ref[:, pl.ds(start, share_rows)])
    return jnp.concatenate(found, axis=1)


def near_product(merged, share, near_pieces, opposite_pieces, lines):
    rows, _ = merged.shape
    share_rows, columns = share.shape

    def body(merged_ref, share_ref, *refs):
        near_refs, opposite_refs, out_ref = refs[:4], refs[4:6], refs[6]
        line, side, lane = place_of_device()

        def product(from_line, *parts):
            return jnp.dot(
                columns_of(merged_ref, from_line, (side, 1 - side), share_rows),
                jnp.concatenate(parts, axis=0),
                preferred_element_type=jnp.float32,
            )

        for which in range(2):

            @pl.when(lane == which)
            def _():
                out_ref[...] = product(line, share_ref[...], opposite_refs[which][...])

        for which in range(2):
            at_lane = (lane, 1 - lane)[which]
            from_line = line - 1 + 2 * at_lane

            @pl.when((from_line >= 0) & (from_line < lines))
            def _():
                out_ref[...] += product(from_line, near_refs[which][...], near_refs[2 + which][...])

    vmem = pl.BlockSpec(memory_space=pltpu.VMEM)
    return pl.pallas_call(
        body,
        in_specs=[vmem] * 8,
        out_specs=vmem,
        out_shape=jax.ShapeDtypeStruct((rows, columns), jnp.float32),
        compiler_params=pltpu.CompilerParams(vmem_limit_bytes=16 << 20),
        name="near_product",
    )(merged, share, *near_pieces, *opposite_pieces)


def far_product(merged, near_sum, far_pieces, lines):
    rows, _ = merged.shape
    share_rows, columns = far_pieces[0].shape
    chunk = 512

    def body(merged_ref, near_ref, *refs):
        piece_refs, out_hbm, rounded, sent = refs[:4], refs[4], refs[5], refs[6]
        line, side, lane = place_of_device()
        first_side = jnp.where(lax.axis_index("tp") // 2 % 2 == 1, 1 - side, side)
        before = jnp.maximum(line - 1, 0)

        def other_line(index):
            found = jnp.where(index < before, index, line + 2 + index - before)
            return jnp.where(found < lines, found, -1)

        sources = [other_line(lane), other_line(1 - lane)]

        def finish(slots):
            left = [
                columns_of(merged_ref, sources[slot], (first_side, 1 - first_side), share_rows)
                for slot in slots
            ]
            left = jnp.concatenate(left, axis=1) if left else None
            copies = []
            for first in range(0, columns, chunk):
                here = slice(first, first + chunk)
                total = near_ref[:, here]
                if slots:
                    right = [piece_refs[2 * i + slot][:, here] for slot in slots for i in range(2)]
                    total = total + jnp.dot(
                        left, jnp.concatenate(right, axis=0), preferred_element_type=jnp.float32
                    )
                rounded[:, here] = total.astype(rounded.dtype)
                copies.append(
                    pltpu.make_async_copy(
                        rounded.at[:, pl.ds(first, chunk)],
                        out_hbm.at[:, pl.ds(first, chunk)],
                        sent.at[first // chunk],
                    )
                )
                copies[-1].start()
            for copy in copies:
                copy.wait()

        for slots in ((0, 1), (0,), (1,), ()):
            wanted = [(sources[slot] >= 0) == (slot in slots) for slot in range(2)]

            @pl.when(wanted[0] & wanted[1])
            def _():
                finish(slots)

    vmem = pl.BlockSpec(memory_space=pltpu.VMEM)
    return pl.pallas_call(
        body,
        in_specs=[vmem] * 6,
        out_specs=pl.BlockSpec(memory_space=pl.ANY),
        out_shape=pltpu.HBM((rows, columns), jnp.bfloat16),
        scratch_shapes=[
            pltpu.VMEM((rows, columns), jnp.bfloat16),
            pltpu.SemaphoreType.DMA((columns // chunk,)),
        ],
        compiler_params=pltpu.CompilerParams(vmem_limit_bytes=16 << 20),
        name="far_product",
    )(merged, near_sum, *far_pieces)


def on_device(
    tokens,
    norm_gain,
    query_weight,
    key_weight,
    value_weight,
    sink_logits,
    conv_in_weight,
    conv_gate_weight,
    conv_taps,
    conv_gain,
    point_weight,
    output_gain,
    output_weight,
):
    sp_size, tp_size = lax.axis_size("sp"), lax.axis_size("tp")
    lines = sp_size // 2
    by_shares = sends_shares(sp_size, tp_size)
    if by_shares:
        routes = ShareRoutes(lines, tp_size)
        near = routes.send(output_weight, routes.beside)
        far = routes.send(output_weight, routes.beyond)
    *last_rows, tail, joined, other_tokens = project_last(
        tokens, norm_gain, query_weight, key_weight, value_weight, conv_in_weight, conv_gate_weight
    )
    earlier = from_behind(tail, "sp", 1)
    pair_width = key_weight.shape[1] + value_weight.shape[1]
    first_rows = project_rest(other_tokens, norm_gain, joined, query_weight.shape[1], pair_width)
    mixed = mix_rows(first_rows, last_rows, earlier, sink_logits, conv_taps, tp_size)
    exchanged = lax.all_to_all(mixed, "tp", split_axis=0, concat_axis=0, tiled=True)
    merged = merge_mixers(exchanged, conv_gain, point_weight, output_gain)
    if by_shares:
        opposite = routes.send(output_weight, routes.lower_lane_across)
        near_across = routes.send(near, routes.holders_across)
        far_other = routes.send(far, routes.to_neighbours)
        near_pieces = near, routes.send(near, routes.lanes)
        near_pieces += near_across, routes.send(near_across, routes.lanes)
        opposite_pieces = opposite, routes.send(opposite, routes.upper_lane_from_lower)
        far_pieces = far, routes.send(far, routes.lanes)
        far_pieces += far_other, routes.send(far_other, routes.lanes)
        near_sum = near_product(merged, output_weight, near_pieces, opposite_pieces, lines)
        return far_product(merged, near_sum, far_pieces, lines)
    projected = jnp.dot(
        merged,
        lax.all_gather(output_weight, "sp", axis=0, tiled=True),
        preferred_element_type=jnp.float32,
    )
    return projected.astype(jnp.bfloat16)


def sends_shares(sp_size, tp_size):
    return sp_size % 2 == 0 and tp_size % 4 == 0 and 3 <= sp_size // 2 <= 4


def solution(mesh):
    in_specs = (
        P("sp", None),
        P(),
        P(None, "tp"),
        P(None, "tp"),
        P(None, "tp"),
        P("tp"),
        P(None, "tp"),
        P(None, "tp"),
        P(),
        P(),
        P(),
        P(),
        P("sp", None),
    )
    out_specs = P(("sp", "tp"), None)
    return jax.shard_map(
        on_device, mesh=mesh, in_specs=in_specs, out_specs=out_specs, check_vma=False
    )
```

```python
import jax
import jax.numpy as jnp
from jax import lax
from jax.experimental import pallas as pl
from jax.experimental.pallas import tpu as pltpu
from jax.sharding import PartitionSpec as P


HEAD_DIM = 64
WINDOW = 128
CONV_WIDTH = 31


NORM_EPSILON = 1e-06
MASKED_SCORE = -1e30
HALO = 32


PLACE = ("sp", "tp")


def from_behind(block, axis, distance):
    devices = range(lax.axis_size(axis))
    route = [(i - distance, i) for i in devices if i - distance in devices]
    return lax.ppermute(block, axis, route)


BLOCK = 256


def normed_rows(token_rows, gain):
    widened = token_rows.astype(jnp.float32)
    scale = lax.rsqrt(jnp.mean(widened * widened, axis=-1, keepdims=True) + NORM_EPSILON)
    return (widened * scale * gain).astype(jnp.bfloat16)


def split_product(normed, joined, heads_width, pair_width, channels):
    result = jnp.dot(normed, joined, preferred_element_type=jnp.float32)
    pairs_end = heads_width + pair_width
    conv_in = result[:, pairs_end : pairs_end + channels]
    gated = conv_in * jax.nn.sigmoid(result[:, pairs_end + channels :])
    return [
        part.astype(jnp.bfloat16)
        for part in (result[:, :heads_width], result[:, heads_width:pairs_end], gated)
    ]


def project_last(tokens, norm_gain, query_weight, key_weight, value_weight, in_weight, gate_weight):
    rows, width = tokens.shape
    heads_width, key_width, channels = query_weight.shape[1], key_weight.shape[1], in_weight.shape[1]
    pair_width = key_width + value_weight.shape[1]
    tail = WINDOW + HALO
    others = rows - BLOCK
    starts = [0, heads_width + pair_width, heads_width + pair_width + channels]

    def body(
        gain_hbm, tokens_hbm, query_hbm, key_hbm, value_hbm, in_hbm, gate_hbm,
        queries_ref, pairs_ref, gated_ref, tail_ref, joined, rest_ref,
        last_ref, pairs_rows, gain_ref, arrived,
    ):
        copies = [
            pltpu.make_async_copy(source, target, arrived.at[i])
            for i, (source, target) in enumerate(
                [
                    (gain_hbm, gain_ref),
                    (tokens_hbm.at[pl.ds(others, BLOCK)], last_ref),
                    (key_hbm, pairs_rows.at[pl.ds(0, key_width)]),
                    (value_hbm, pairs_rows.at[pl.ds(key_width, pair_width - key_width)]),
                ]
                + [
                    (source, joined.at[:, pl.ds(start, source.shape[1])])
                    for source, start in zip([query_hbm, in_hbm, gate_hbm], starts)
                ]
                + [(tokens_hbm.at[pl.ds(0, others)], rest_ref)]
            )
        ]
        for copy in copies:
            copy.start()
        for copy in copies[:2]:
            copy.wait()
        normed = normed_rows(last_ref[...], gain_ref[...])
        for copy in copies[2:4]:
            copy.wait()
        joined[:, heads_width : heads_width + pair_width] = pairs_rows[...].T
        for copy in copies[4:7]:
            copy.wait()
        queries, pairs, gated = split_product(
            normed, joined[...], heads_width, pair_width, channels
        )
        queries_ref[...] = queries
        pairs_ref[...] = pairs
        gated_ref[...] = gated
        tail_ref[:WINDOW] = pairs[BLOCK - WINDOW :]
        tail_ref[WINDOW:] = gated[BLOCK - HALO :]
        copies[7].wait()

    vmem = pl.BlockSpec(memory_space=pltpu.VMEM)
    in_hbm = [
        pltpu.with_memory_space_constraint(operand, pltpu.HBM)
        for operand in (
            norm_gain[None], tokens, query_weight, key_weight.T, value_weight.T, in_weight,
            gate_weight,
        )
    ]
    shapes = [
        (BLOCK, heads_width), (BLOCK, pair_width), (BLOCK, channels), (tail, channels),
        (width, heads_width + pair_width + 2 * channels), (others, width),
    ]
    return pl.pallas_call(
        body,
        in_specs=[pl.BlockSpec(memory_space=pl.ANY)] * 7,
        out_specs=[vmem] * len(shapes),
        out_shape=[jax.ShapeDtypeStruct(shape, jnp.bfloat16) for shape in shapes],
        scratch_shapes=[
            pltpu.VMEM((BLOCK, width), jnp.bfloat16),
            pltpu.VMEM((pair_width, width), jnp.bfloat16),
            pltpu.VMEM((1, width), jnp.float32),
            pltpu.SemaphoreType.DMA((8,)),
        ],
        compiler_params=pltpu.CompilerParams(vmem_limit_bytes=20 << 20),
        name="project_last",
    )(*in_hbm)


def project_rest(tokens, norm_gain, joined, heads_width, pair_width):
    rows, width = tokens.shape
    channels = (joined.shape[1] - heads_width - pair_width) // 2
    blocks = rows // BLOCK

    def body(gain_ref, tokens_ref, joined_ref, queries_ref, pairs_ref, gated_ref, normed):
        normed[0] = normed_rows(tokens_ref[:BLOCK], gain_ref[...])
        for i in range(blocks):
            here = slice(i * BLOCK, (i + 1) * BLOCK)
            queries, pairs, gated = split_product(
                normed[i], joined_ref[...], heads_width, pair_width, channels
            )
            if i + 1 < blocks:
                following = tokens_ref[(i + 1) * BLOCK : (i + 2) * BLOCK]
                normed[i + 1] = normed_rows(following, gain_ref[...])
            queries_ref[here] = queries
            pairs_ref[here] = pairs
            gated_ref[here] = gated

    vmem = pl.BlockSpec(memory_space=pltpu.VMEM)
    return pl.pallas_call(
        body,
        in_specs=[vmem] * 3,
        out_specs=[vmem] * 3,
        out_shape=[
            jax.ShapeDtypeStruct((rows, columns), jnp.bfloat16)
            for columns in (heads_width, pair_width, channels)
        ],
        scratch_shapes=[pltpu.VMEM((blocks, BLOCK, width), jnp.bfloat16)],
        compiler_params=pltpu.CompilerParams(vmem_limit_bytes=24 << 20),
        name="project_rest",
    )(norm_gain[None], tokens, joined)


def mix_rows(first_rows, last_rows, earlier, sinks, taps, shares):
    rest, heads_width = first_rows[0].shape
    rows = rest + last_rows[0].shape[0]
    pair_width, channels = first_rows[1].shape[1], first_rows[2].shape[1]
    head_count = heads_width // HEAD_DIM
    share_rows = rows // shares

    def body(
        sinks_ref, queries_ref, pairs_ref, gated_ref, last_queries, last_pairs, last_gated,
        earlier_ref, taps_ref, out_ref, band, extended,
    ):
        band[:WINDOW] = earlier_ref[:WINDOW]
        band[WINDOW : WINDOW + rest] = pairs_ref[...]
        band[WINDOW + rest :] = last_pairs[...]
        extended[:HALO] = earlier_ref[WINDOW:].astype(jnp.float32)
        extended[HALO : HALO + rest] = gated_ref[...].astype(jnp.float32)
        extended[HALO + rest :] = last_gated[...].astype(jnp.float32)
        query_index = lax.broadcasted_iota(jnp.int32, (WINDOW, 2 * WINDOW), 0)
        key_index = lax.broadcasted_iota(jnp.int32, (WINDOW, 2 * WINDOW), 1)
        distance = WINDOW + query_index - key_index
        in_window = (distance >= 0) & (distance < WINDOW)
        not_before = in_window & ((lax.axis_index("sp") > 0) | (key_index >= WINDOW))
        own = pl.multiple_of(lax.axis_index("tp") * channels, channels)
        tap_rows = taps_ref[:, pl.ds(own, channels)].astype(jnp.float32)
        for block in range(rows // WINDOW):
            start = block * WINDOW
            share, inner = start // share_rows, start % share_rows
            keys = band[start : start + 2 * WINDOW, :HEAD_DIM]
            values = band[start : start + 2 * WINDOW, HEAD_DIM : 2 * HEAD_DIM]
            allowed = not_before if block == 0 else in_window
            found = []
            for head in range(head_count):
                source, at = (queries_ref, start) if start < rest else (last_queries, start - rest)
                here = source[at : at + WINDOW, head * HEAD_DIM : (head + 1) * HEAD_DIM]
                scores = lax.dot_general(
                    here, keys, (((1,), (1,)), ((), ())), preferred_element_type=jnp.float32
                ) * HEAD_DIM ** (-0.5)
                scores = jnp.where(allowed, scores, MASKED_SCORE)
                sink = sinks_ref[head]
                peak = jnp.maximum(jnp.max(scores, axis=-1, keepdims=True), sink)
                raised = jnp.exp(scores - peak)
                denominator = jnp.sum(raised, axis=-1, keepdims=True) + jnp.exp(sink - peak)
                weights = (raised * (1.0 / denominator)).astype(jnp.bfloat16)
                found.append(
                    jnp.dot(weights, values, preferred_element_type=jnp.float32).astype(jnp.bfloat16)
                )
            out_ref[share, inner : inner + WINDOW, :heads_width] = jnp.concatenate(found, axis=1)
            total = jnp.zeros((WINDOW, channels), jnp.float32)
            for tap in range(CONV_WIDTH):
                from_row = start + HALO - (CONV_WIDTH - 1) + tap
                total = total + tap_rows[tap : tap + 1] * extended[from_row : from_row + WINDOW]
            out_ref[share, inner : inner + WINDOW, heads_width:] = total.astype(jnp.bfloat16)

    whole = pl.BlockSpec(memory_space=pltpu.VMEM)
    scalars = pl.BlockSpec(memory_space=pltpu.SMEM)
    return pl.pallas_call(
        body,
        in_specs=[scalars] + [whole] * 8,
        out_specs=whole,
        out_shape=jax.ShapeDtypeStruct((shares, share_rows, heads_width + channels), jnp.bfloat16),
        scratch_shapes=[
            pltpu.VMEM((WINDOW + rows, pair_width), jnp.bfloat16),
            pltpu.VMEM((HALO + rows, channels), jnp.float32),
        ],
        compiler_params=pltpu.CompilerParams(vmem_limit_bytes=12 << 20),
        name="mix_rows",
    )(sinks, *first_rows, *last_rows, earlier, taps)


def merge_mixers(exchanged, conv_gain, point_weight, output_gain):
    shares, rows, joint = exchanged.shape
    heads_width = joint // 2
    width = shares * heads_width

    def body(exchanged_ref, conv_gain_ref, gain_ref, point_hbm, out_ref, point_ref, fetched):
        fetch = pltpu.make_async_copy(point_hbm, point_ref, fetched)
        fetch.start()
        attended = jnp.concatenate(
            [exchanged_ref[i, :, :heads_width] for i in range(shares)], axis=1
        ).astype(jnp.float32)
        convolved = jnp.concatenate(
            [exchanged_ref[i, :, heads_width:] for i in range(shares)], axis=1
        ).astype(jnp.float32)
        centered = convolved - jnp.mean(convolved, axis=-1, keepdims=True)
        scaled = (
            centered
            * lax.rsqrt(jnp.mean(centered * centered, axis=-1, keepdims=True) + NORM_EPSILON)
            * conv_gain_ref[...]
        )
        activated = (scaled * jax.nn.sigmoid(scaled)).astype(jnp.bfloat16)
        out_ref[:, :width] = (
            attended
            * lax.rsqrt(jnp.mean(attended * attended, axis=-1, keepdims=True) + NORM_EPSILON)
            * gain_ref[:, :width]
        ).astype(jnp.bfloat16)
        fetch.wait()
        pointwise = jnp.dot(activated, point_ref[...], preferred_element_type=jnp.float32)
        out_ref[:, width:] = (
            pointwise
            * lax.rsqrt(jnp.mean(pointwise * pointwise, axis=-1, keepdims=True) + NORM_EPSILON)
            * gain_ref[:, width:]
        ).astype(jnp.bfloat16)

    vmem = pl.BlockSpec(memory_space=pltpu.VMEM)
    return pl.pallas_call(
        body,
        in_specs=[vmem] * 3 + [pl.BlockSpec(memory_space=pl.ANY)],
        out_specs=vmem,
        out_shape=jax.ShapeDtypeStruct((rows, output_gain.shape[0]), jnp.bfloat16),
        scratch_shapes=[
            pltpu.VMEM(point_weight.shape, point_weight.dtype),
            pltpu.SemaphoreType.DMA(()),
        ],
        compiler_params=pltpu.CompilerParams(vmem_limit_bytes=12 << 20),
        name="merge_mixers",
    )(
        exchanged, conv_gain[None], output_gain[None],
        pltpu.with_memory_space_constraint(point_weight, pltpu.HBM),
    )


class ShareRoutes:
    def __init__(self, lines, tp_size):
        self.lines, self.tp_size = lines, tp_size

    def number(self, line, side, lane):
        return (line * 2 + side) * self.tp_size + lane

    def send(self, block, target):
        found = []
        for line in range(self.lines):
            for side in range(2):
                for lane in range(self.tp_size):
                    to = target(line, side, lane)
                    if 0 <= to[0] < self.lines:
                        found.append((self.number(line, side, lane), self.number(*to)))
        return lax.ppermute(block, PLACE, found)

    def beside(self, line, side, lane):
        to_line = line + 1 if lane % 2 == 0 else line - 1
        if 0 <= to_line < self.lines:
            return to_line, side, lane
        return line, 1 - side, lane ^ 1

    def beyond(self, line, side, lane):
        targets = far_lines(line, self.lines)
        if lane % 2 >= len(targets):
            return -1, side, lane
        to_line = targets[lane % 2]
        to_side = 1 - side if lane // 2 % 2 else side
        to_lane = lane - lane % 2 + far_lines(to_line, self.lines).index(line)
        return to_line, to_side, to_lane

    def holders_across(self, line, side, lane):
        from_line = line - 1 if lane % 2 == 0 else line + 1
        return (line if 0 <= from_line < self.lines else -1), 1 - side, lane

    def inner(self, line, lane):
        return line if 0 < line < self.lines - 1 and lane % 2 == 0 else -1

    def inner_across(self, line, side, lane):
        return self.inner(line, lane), 1 - side, lane

    def inner_upper(self, line, side, lane):
        return self.inner(line, lane), side, lane ^ 1

    def to_neighbours(self, line, side, lane):
        held = lane % 2 < len(far_lines(line, self.lines))
        to = (1 - side, lane) if lane % 2 == 0 else (side, lane ^ 2)
        return (line if held else -1), *to

    def lanes(self, line, side, lane):
        return line, side, lane ^ 1


def far_lines(line, lines):
    return [other for other in range(lines) if abs(other - line) > 1]


def place_of_device():
    position, lane = lax.axis_index("sp"), lax.axis_index("tp") % 2
    return position // 2, position % 2, lane


def columns_of(merged_ref, from_line, sides, share_rows):
    found = []
    for at_side in sides:
        start = pl.multiple_of((from_line * 2 + at_side) * share_rows, share_rows)
        found.append(merged_ref[:, pl.ds(start, share_rows)])
    return jnp.concatenate(found, axis=1)


def far_line(line, at_lane, lines):
    before = jnp.maximum(line - 1, 0)
    found = jnp.where(at_lane < before, at_lane, line + 2 + at_lane - before)
    return jnp.where(found < lines, found, -1)


def odd_row():
    return lax.axis_index("tp") // 2 % 2


def early_product(merged, share, near_pieces, opposite_pieces, far_pieces, lines):
    rows, _ = merged.shape
    share_rows, columns = share.shape

    def body(merged_ref, share_ref, *refs):
        near_refs, opposite_refs, far_refs, out_ref = refs[:4], refs[4:6], refs[6:8], refs[8]
        line, side, lane = place_of_device()

        def product(from_line, sides, *parts):
            return jnp.dot(
                columns_of(merged_ref, from_line, sides, share_rows),
                jnp.concatenate(parts, axis=0),
                preferred_element_type=jnp.float32,
            )

        both_sides = (side, 1 - side)
        at_end = (line == 0) | (line == lines - 1)
        holder = jnp.where(line == lines - 1, 1, 0)
        for which in range(2):
            held = holder == (lane, 1 - lane)[which]
            for ends, ref in ((True, near_refs[which]), (False, opposite_refs[which])):

                @pl.when(held & (at_end == ends))
                def _():
                    out_ref[...] = product(line, both_sides, share_ref[...], ref[...])

        for which in range(2):
            at_lane = (lane, 1 - lane)[which]
            from_line = line - 1 + 2 * at_lane

            @pl.when((from_line >= 0) & (from_line < lines))
            def _():
                out_ref[...] += product(
                    from_line, both_sides, near_refs[which][...], near_refs[2 + which][...]
                )

        first_side = jnp.where(odd_row() == 1, 1 - side, side)
        for which in range(2):
            from_line = far_line(line, (lane, 1 - lane)[which], lines)

            @pl.when(from_line >= 0)
            def _():
                out_ref[...] += product(from_line, (first_side,), far_refs[which][...])

    vmem = pl.BlockSpec(memory_space=pltpu.VMEM)
    return pl.pallas_call(
        body,
        in_specs=[vmem] * 10,
        out_specs=vmem,
        out_shape=jax.ShapeDtypeStruct((rows, columns), jnp.float32),
        compiler_params=pltpu.CompilerParams(vmem_limit_bytes=16 << 20),
        name="early_product",
    )(merged, share, *near_pieces, *opposite_pieces, *far_pieces)


def late_product(merged, early_sum, far_pieces, lines):
    rows, _ = merged.shape
    share_rows, columns = far_pieces[0].shape
    chunk = 512

    def body(merged_ref, early_ref, *refs):
        far_refs, out_hbm, rounded, sent = refs[:2], refs[2], refs[3], refs[4]
        line, side, lane = place_of_device()
        last_side = jnp.where(odd_row() == 1, side, 1 - side)
        sources = [far_line(line, lane, lines), far_line(line, 1 - lane, lines)]

        def finish(slots):
            if slots:
                left = [
                    columns_of(merged_ref, sources[slot], (last_side,), share_rows)
                    for slot in slots
                ]
                left = jnp.concatenate(left, axis=1)
            copies = []
            for first in range(0, columns, chunk):
                here = slice(first, first + chunk)
                total = early_ref[:, here]
                if slots:
                    right = jnp.concatenate([far_refs[slot][:, here] for slot in slots], axis=0)
                    total = total + jnp.dot(left, right, preferred_element_type=jnp.float32)
                rounded[:, here] = total.astype(rounded.dtype)
                copies.append(
                    pltpu.make_async_copy(
                        rounded.at[:, pl.ds(first, chunk)],
                        out_hbm.at[:, pl.ds(first, chunk)],
                        sent.at[first // chunk],
                    )
                )
                copies[-1].start()
            for copy in copies:
                copy.wait()

        for slots in ((0, 1), (0,), (1,), ()):
            wanted = [(sources[slot] >= 0) == (slot in slots) for slot in range(2)]

            @pl.when(wanted[0] & wanted[1])
            def _():
                finish(slots)

    vmem = pl.BlockSpec(memory_space=pltpu.VMEM)
    return pl.pallas_call(
        body,
        in_specs=[vmem] * 4,
        out_specs=pl.BlockSpec(memory_space=pl.ANY),
        out_shape=pltpu.HBM((rows, columns), jnp.bfloat16),
        scratch_shapes=[
            pltpu.VMEM((rows, columns), jnp.bfloat16),
            pltpu.SemaphoreType.DMA((columns // chunk,)),
        ],
        compiler_params=pltpu.CompilerParams(vmem_limit_bytes=16 << 20),
        name="late_product",
    )(merged, early_sum, *far_pieces)


def on_device(
    tokens,
    norm_gain,
    query_weight,
    key_weight,
    value_weight,
    sink_logits,
    conv_in_weight,
    conv_gate_weight,
    conv_taps,
    conv_gain,
    point_weight,
    output_gain,
    output_weight,
):
    sp_size, tp_size = lax.axis_size("sp"), lax.axis_size("tp")
    lines = sp_size // 2
    by_shares = sends_shares(sp_size, tp_size)
    if by_shares:
        routes = ShareRoutes(lines, tp_size)
        near = routes.send(output_weight, routes.beside)
        far = routes.send(output_weight, routes.beyond)
    *last_rows, tail, joined, other_tokens = project_last(
        tokens, norm_gain, query_weight, key_weight, value_weight, conv_in_weight, conv_gate_weight
    )
    earlier = from_behind(tail, "sp", 1)
    pair_width = key_weight.shape[1] + value_weight.shape[1]
    first_rows = project_rest(other_tokens, norm_gain, joined, query_weight.shape[1], pair_width)
    mixed = mix_rows(first_rows, last_rows, earlier, sink_logits, conv_taps, tp_size)
    exchanged = lax.all_to_all(mixed, "tp", split_axis=0, concat_axis=0, tiled=True)
    merged = merge_mixers(exchanged, conv_gain, point_weight, output_gain)
    if by_shares:
        opposite = routes.send(output_weight, routes.inner_across)
        near_across = routes.send(near, routes.holders_across)
        far_other = routes.send(far, routes.to_neighbours)
        near_pieces = near, routes.send(near, routes.lanes)
        near_pieces += near_across, routes.send(near_across, routes.lanes)
        opposite_pieces = opposite, routes.send(opposite, routes.inner_upper)
        far_pieces = far, routes.send(far, routes.lanes)
        last_pieces = far_other, routes.send(far_other, routes.lanes)
        early_sum = early_product(
            merged, output_weight, near_pieces, opposite_pieces, far_pieces, lines
        )
        return late_product(merged, early_sum, last_pieces, lines)
    projected = jnp.dot(
        merged,
        lax.all_gather(output_weight, "sp", axis=0, tiled=True),
        preferred_element_type=jnp.float32,
    )
    return projected.astype(jnp.bfloat16)


def sends_shares(sp_size, tp_size):
    return sp_size % 2 == 0 and tp_size % 4 == 0 and 3 <= sp_size // 2 <= 4


def solution(mesh):
    in_specs = (
        P("sp", None),
        P(),
        P(None, "tp"),
        P(None, "tp"),
        P(None, "tp"),
        P("tp"),
        P(None, "tp"),
        P(None, "tp"),
        P(),
        P(),
        P(),
        P(),
        P("sp", None),
    )
    out_specs = P(("sp", "tp"), None)
    return jax.shard_map(
        on_device, mesh=mesh, in_specs=in_specs, out_specs=out_specs, check_vma=False
    )
```

```python
import jax
import jax.numpy as jnp
from jax import lax
from jax.experimental import pallas as pl
from jax.experimental.pallas import tpu as pltpu
from jax.sharding import PartitionSpec as P


HEAD_DIM = 64
WINDOW = 128
CONV_WIDTH = 31


NORM_EPSILON = 1e-06
MASKED_SCORE = -1e30
HALO = 32


PLACE = ("sp", "tp")


def from_behind(block, axis, distance):
    devices = range(lax.axis_size(axis))
    route = [(i - distance, i) for i in devices if i - distance in devices]
    return lax.ppermute(block, axis, route)


BLOCK = 256


def normed_rows(token_rows, gain):
    widened = token_rows.astype(jnp.float32)
    scale = lax.rsqrt(jnp.mean(widened * widened, axis=-1, keepdims=True) + NORM_EPSILON)
    return (widened * scale * gain).astype(jnp.bfloat16)


def split_product(normed, joined, heads_width, pair_width, channels):
    result = jnp.dot(normed, joined, preferred_element_type=jnp.float32)
    pairs_end = heads_width + pair_width
    conv_in = result[:, pairs_end : pairs_end + channels]
    gated = conv_in * jax.nn.sigmoid(result[:, pairs_end + channels :])
    return [
        part.astype(jnp.bfloat16)
        for part in (result[:, :heads_width], result[:, heads_width:pairs_end], gated)
    ]


def project_last(tokens, norm_gain, query_weight, key_weight, value_weight, in_weight, gate_weight):
    rows, width = tokens.shape
    heads_width, key_width, channels = query_weight.shape[1], key_weight.shape[1], in_weight.shape[1]
    pair_width = key_width + value_weight.shape[1]
    tail = WINDOW + HALO
    others = rows - BLOCK
    starts = [0, heads_width + pair_width, heads_width + pair_width + channels]

    def body(
        gain_hbm, tokens_hbm, query_hbm, key_hbm, value_hbm, in_hbm, gate_hbm,
        queries_ref, pairs_ref, gated_ref, tail_ref, joined, rest_ref,
        last_ref, pairs_rows, gain_ref, arrived,
    ):
        copies = [
            pltpu.make_async_copy(source, target, arrived.at[i])
            for i, (source, target) in enumerate(
                [
                    (gain_hbm, gain_ref),
                    (tokens_hbm.at[pl.ds(others, BLOCK)], last_ref),
                    (key_hbm, pairs_rows.at[pl.ds(0, key_width)]),
                    (value_hbm, pairs_rows.at[pl.ds(key_width, pair_width - key_width)]),
                ]
                + [
                    (source, joined.at[:, pl.ds(start, source.shape[1])])
                    for source, start in zip([query_hbm, in_hbm, gate_hbm], starts)
                ]
                + [(tokens_hbm.at[pl.ds(0, others)], rest_ref)]
            )
        ]
        for copy in copies:
            copy.start()
        for copy in copies[:2]:
            copy.wait()
        normed = normed_rows(last_ref[...], gain_ref[...])
        for copy in copies[2:4]:
            copy.wait()
        joined[:, heads_width : heads_width + pair_width] = pairs_rows[...].T
        for copy in copies[4:7]:
            copy.wait()
        queries, pairs, gated = split_product(
            normed, joined[...], heads_width, pair_width, channels
        )
        queries_ref[...] = queries
        pairs_ref[...] = pairs
        gated_ref[...] = gated
        tail_ref[:WINDOW] = pairs[BLOCK - WINDOW :]
        tail_ref[WINDOW:] = gated[BLOCK - HALO :]
        copies[7].wait()

    vmem = pl.BlockSpec(memory_space=pltpu.VMEM)
    in_hbm = [
        pltpu.with_memory_space_constraint(operand, pltpu.HBM)
        for operand in (
            norm_gain[None], tokens, query_weight, key_weight.T, value_weight.T, in_weight,
            gate_weight,
        )
    ]
    shapes = [
        (BLOCK, heads_width), (BLOCK, pair_width), (BLOCK, channels), (tail, channels),
        (width, heads_width + pair_width + 2 * channels), (others, width),
    ]
    return pl.pallas_call(
        body,
        in_specs=[pl.BlockSpec(memory_space=pl.ANY)] * 7,
        out_specs=[vmem] * len(shapes),
        out_shape=[jax.ShapeDtypeStruct(shape, jnp.bfloat16) for shape in shapes],
        scratch_shapes=[
            pltpu.VMEM((BLOCK, width), jnp.bfloat16),
            pltpu.VMEM((pair_width, width), jnp.bfloat16),
            pltpu.VMEM((1, width), jnp.float32),
            pltpu.SemaphoreType.DMA((8,)),
        ],
        compiler_params=pltpu.CompilerParams(vmem_limit_bytes=20 << 20),
        name="project_last",
    )(*in_hbm)


def project_rest(tokens, norm_gain, joined, heads_width, pair_width):
    rows, width = tokens.shape
    channels = (joined.shape[1] - heads_width - pair_width) // 2
    blocks = rows // BLOCK

    def body(gain_ref, tokens_ref, joined_ref, queries_ref, pairs_ref, gated_ref, normed):
        normed[0] = normed_rows(tokens_ref[:BLOCK], gain_ref[...])
        for i in range(blocks):
            here = slice(i * BLOCK, (i + 1) * BLOCK)
            queries, pairs, gated = split_product(
                normed[i], joined_ref[...], heads_width, pair_width, channels
            )
            if i + 1 < blocks:
                following = tokens_ref[(i + 1) * BLOCK : (i + 2) * BLOCK]
                normed[i + 1] = normed_rows(following, gain_ref[...])
            queries_ref[here] = queries
            pairs_ref[here] = pairs
            gated_ref[here] = gated

    vmem = pl.BlockSpec(memory_space=pltpu.VMEM)
    return pl.pallas_call(
        body,
        in_specs=[vmem] * 3,
        out_specs=[vmem] * 3,
        out_shape=[
            jax.ShapeDtypeStruct((rows, columns), jnp.bfloat16)
            for columns in (heads_width, pair_width, channels)
        ],
        scratch_shapes=[pltpu.VMEM((blocks, BLOCK, width), jnp.bfloat16)],
        compiler_params=pltpu.CompilerParams(vmem_limit_bytes=24 << 20),
        name="project_rest",
    )(norm_gain[None], tokens, joined)


def mix_rows(first_rows, last_rows, earlier, sinks, taps, shares):
    rest, heads_width = first_rows[0].shape
    rows = rest + last_rows[0].shape[0]
    pair_width, channels = first_rows[1].shape[1], first_rows[2].shape[1]
    head_count = heads_width // HEAD_DIM
    share_rows = rows // shares

    def body(
        sinks_ref, queries_ref, pairs_ref, gated_ref, last_queries, last_pairs, last_gated,
        earlier_ref, taps_ref, out_ref, band, extended,
    ):
        band[:WINDOW] = earlier_ref[:WINDOW]
        band[WINDOW : WINDOW + rest] = pairs_ref[...]
        band[WINDOW + rest :] = last_pairs[...]
        extended[:HALO] = earlier_ref[WINDOW:].astype(jnp.float32)
        extended[HALO : HALO + rest] = gated_ref[...].astype(jnp.float32)
        extended[HALO + rest :] = last_gated[...].astype(jnp.float32)
        query_index = lax.broadcasted_iota(jnp.int32, (WINDOW, 2 * WINDOW), 0)
        key_index = lax.broadcasted_iota(jnp.int32, (WINDOW, 2 * WINDOW), 1)
        distance = WINDOW + query_index - key_index
        in_window = (distance >= 0) & (distance < WINDOW)
        not_before = in_window & ((lax.axis_index("sp") > 0) | (key_index >= WINDOW))
        own = pl.multiple_of(lax.axis_index("tp") * channels, channels)
        tap_rows = taps_ref[:, pl.ds(own, channels)].astype(jnp.float32)
        for block in range(rows // WINDOW):
            start = block * WINDOW
            share, inner = start // share_rows, start % share_rows
            keys = band[start : start + 2 * WINDOW, :HEAD_DIM]
            values = band[start : start + 2 * WINDOW, HEAD_DIM : 2 * HEAD_DIM]
            allowed = not_before if block == 0 else in_window
            found = []
            for head in range(head_count):
                source, at = (queries_ref, start) if start < rest else (last_queries, start - rest)
                here = source[at : at + WINDOW, head * HEAD_DIM : (head + 1) * HEAD_DIM]
                scores = lax.dot_general(
                    here, keys, (((1,), (1,)), ((), ())), preferred_element_type=jnp.float32
                ) * HEAD_DIM ** (-0.5)
                scores = jnp.where(allowed, scores, MASKED_SCORE)
                sink = sinks_ref[head]
                peak = jnp.maximum(jnp.max(scores, axis=-1, keepdims=True), sink)
                raised = jnp.exp(scores - peak)
                denominator = jnp.sum(raised, axis=-1, keepdims=True) + jnp.exp(sink - peak)
                weights = (raised * (1.0 / denominator)).astype(jnp.bfloat16)
                found.append(
                    jnp.dot(weights, values, preferred_element_type=jnp.float32).astype(jnp.bfloat16)
                )
            out_ref[share, inner : inner + WINDOW, :heads_width] = jnp.concatenate(found, axis=1)
            total = jnp.zeros((WINDOW, channels), jnp.float32)
            for tap in range(CONV_WIDTH):
                from_row = start + HALO - (CONV_WIDTH - 1) + tap
                total = total + tap_rows[tap : tap + 1] * extended[from_row : from_row + WINDOW]
            out_ref[share, inner : inner + WINDOW, heads_width:] = total.astype(jnp.bfloat16)

    whole = pl.BlockSpec(memory_space=pltpu.VMEM)
    scalars = pl.BlockSpec(memory_space=pltpu.SMEM)
    return pl.pallas_call(
        body,
        in_specs=[scalars] + [whole] * 8,
        out_specs=whole,
        out_shape=jax.ShapeDtypeStruct((shares, share_rows, heads_width + channels), jnp.bfloat16),
        scratch_shapes=[
            pltpu.VMEM((WINDOW + rows, pair_width), jnp.bfloat16),
            pltpu.VMEM((HALO + rows, channels), jnp.float32),
        ],
        compiler_params=pltpu.CompilerParams(vmem_limit_bytes=12 << 20),
        name="mix_rows",
    )(sinks, *first_rows, *last_rows, earlier, taps)


def merge_mixers(exchanged, conv_gain, point_weight, output_gain):
    shares, rows, joint = exchanged.shape
    heads_width = joint // 2
    width = shares * heads_width

    def body(exchanged_ref, conv_gain_ref, gain_ref, point_hbm, out_ref, point_ref, fetched):
        fetch = pltpu.make_async_copy(point_hbm, point_ref, fetched)
        fetch.start()
        attended = jnp.concatenate(
            [exchanged_ref[i, :, :heads_width] for i in range(shares)], axis=1
        ).astype(jnp.float32)
        convolved = jnp.concatenate(
            [exchanged_ref[i, :, heads_width:] for i in range(shares)], axis=1
        ).astype(jnp.float32)
        centered = convolved - jnp.mean(convolved, axis=-1, keepdims=True)
        scaled = (
            centered
            * lax.rsqrt(jnp.mean(centered * centered, axis=-1, keepdims=True) + NORM_EPSILON)
            * conv_gain_ref[...]
        )
        activated = (scaled * jax.nn.sigmoid(scaled)).astype(jnp.bfloat16)
        out_ref[:, :width] = (
            attended
            * lax.rsqrt(jnp.mean(attended * attended, axis=-1, keepdims=True) + NORM_EPSILON)
            * gain_ref[:, :width]
        ).astype(jnp.bfloat16)
        fetch.wait()
        pointwise = jnp.dot(activated, point_ref[...], preferred_element_type=jnp.float32)
        out_ref[:, width:] = (
            pointwise
            * lax.rsqrt(jnp.mean(pointwise * pointwise, axis=-1, keepdims=True) + NORM_EPSILON)
            * gain_ref[:, width:]
        ).astype(jnp.bfloat16)

    vmem = pl.BlockSpec(memory_space=pltpu.VMEM)
    return pl.pallas_call(
        body,
        in_specs=[vmem] * 3 + [pl.BlockSpec(memory_space=pl.ANY)],
        out_specs=vmem,
        out_shape=jax.ShapeDtypeStruct((rows, output_gain.shape[0]), jnp.bfloat16),
        scratch_shapes=[
            pltpu.VMEM(point_weight.shape, point_weight.dtype),
            pltpu.SemaphoreType.DMA(()),
        ],
        compiler_params=pltpu.CompilerParams(vmem_limit_bytes=12 << 20),
        name="merge_mixers",
    )(
        exchanged, conv_gain[None], output_gain[None],
        pltpu.with_memory_space_constraint(point_weight, pltpu.HBM),
    )


class ShareRoutes:
    def __init__(self, lines, tp_size):
        self.lines, self.tp_size = lines, tp_size

    def number(self, line, side, lane):
        return (line * 2 + side) * self.tp_size + lane

    def send(self, block, target):
        found = []
        for line in range(self.lines):
            for side in range(2):
                for lane in range(self.tp_size):
                    to = target(line, side, lane)
                    if 0 <= to[0] < self.lines:
                        found.append((self.number(line, side, lane), self.number(*to)))
        return lax.ppermute(block, PLACE, found)

    def beside(self, line, side, lane):
        to_line = line + 1 if lane % 2 == 0 else line - 1
        if 0 <= to_line < self.lines:
            return to_line, side, lane
        return line, 1 - side, lane ^ 1

    def beyond(self, line, side, lane):
        targets = far_lines(line, self.lines)
        if lane % 2 >= len(targets):
            return (line if lane % 2 else -1), 1 - side, lane
        to_line = targets[lane % 2]
        to_side = 1 - side if lane // 2 % 2 else side
        to_lane = lane - lane % 2 + far_lines(to_line, self.lines).index(line)
        return to_line, to_side, to_lane

    def holders_across(self, line, side, lane):
        from_line = line - 1 if lane % 2 == 0 else line + 1
        return (line if 0 <= from_line < self.lines else -1), 1 - side, lane

    def to_neighbours(self, line, side, lane):
        held = lane % 2 < len(far_lines(line, self.lines))
        to = (1 - side, lane) if lane % 2 == 0 else (side, lane ^ 2)
        return (line if held else -1), *to

    def lanes(self, line, side, lane):
        return line, side, lane ^ 1


def far_lines(line, lines):
    return [other for other in range(lines) if abs(other - line) > 1]


def place_of_device():
    position, lane = lax.axis_index("sp"), lax.axis_index("tp") % 2
    return position // 2, position % 2, lane


def columns_of(merged_ref, from_line, sides, share_rows):
    found = []
    for at_side in sides:
        start = pl.multiple_of((from_line * 2 + at_side) * share_rows, share_rows)
        found.append(merged_ref[:, pl.ds(start, share_rows)])
    return jnp.concatenate(found, axis=1)


def far_line(line, at_lane, lines):
    before = jnp.maximum(line - 1, 0)
    found = jnp.where(at_lane < before, at_lane, line + 2 + at_lane - before)
    return jnp.where(found < lines, found, -1)


def odd_row():
    return lax.axis_index("tp") // 2 % 2


def early_product(merged, share, near_pieces, far_pieces, lines):
    rows, _ = merged.shape
    share_rows, columns = share.shape

    def body(merged_ref, share_ref, *refs):
        near_refs, far_refs, out_ref = refs[:4], refs[4:6], refs[6]
        line, side, lane = place_of_device()

        def product(from_line, sides, *parts):
            return jnp.dot(
                columns_of(merged_ref, from_line, sides, share_rows),
                jnp.concatenate(parts, axis=0),
                preferred_element_type=jnp.float32,
            )

        both_sides = (side, 1 - side)
        at_end = (line == 0) | (line == lines - 1)
        holder = jnp.where(line == 0, 0, 1)
        for which in range(2):
            held = holder == (lane, 1 - lane)[which]
            for ends, ref in ((True, near_refs[which]), (False, far_refs[which])):

                @pl.when(held & (at_end == ends))
                def _():
                    out_ref[...] = product(line, both_sides, share_ref[...], ref[...])

        for which in range(2):
            at_lane = (lane, 1 - lane)[which]
            from_line = line - 1 + 2 * at_lane

            @pl.when((from_line >= 0) & (from_line < lines))
            def _():
                out_ref[...] += product(
                    from_line, both_sides, near_refs[which][...], near_refs[2 + which][...]
                )

        first_side = jnp.where(odd_row() == 1, 1 - side, side)
        for which in range(2):
            from_line = far_line(line, (lane, 1 - lane)[which], lines)

            @pl.when(from_line >= 0)
            def _():
                out_ref[...] += product(from_line, (first_side,), far_refs[which][...])

    vmem = pl.BlockSpec(memory_space=pltpu.VMEM)
    return pl.pallas_call(
        body,
        in_specs=[vmem] * 8,
        out_specs=vmem,
        out_shape=jax.ShapeDtypeStruct((rows, columns), jnp.float32),
        compiler_params=pltpu.CompilerParams(vmem_limit_bytes=16 << 20),
        name="early_product",
    )(merged, share, *near_pieces, *far_pieces)


def late_product(merged, early_sum, far_pieces, lines):
    rows, _ = merged.shape
    share_rows, columns = far_pieces[0].shape
    chunk = 512

    def body(merged_ref, early_ref, *refs):
        far_refs, out_hbm, rounded, sent = refs[:2], refs[2], refs[3], refs[4]
        line, side, lane = place_of_device()
        last_side = jnp.where(odd_row() == 1, side, 1 - side)
        sources = [far_line(line, lane, lines), far_line(line, 1 - lane, lines)]

        def finish(slots):
            if slots:
                left = [
                    columns_of(merged_ref, sources[slot], (last_side,), share_rows)
                    for slot in slots
                ]
                left = jnp.concatenate(left, axis=1)
            copies = []
            for first in range(0, columns, chunk):
                here = slice(first, first + chunk)
                total = early_ref[:, here]
                if slots:
                    right = jnp.concatenate([far_refs[slot][:, here] for slot in slots], axis=0)
                    total = total + jnp.dot(left, right, preferred_element_type=jnp.float32)
                rounded[:, here] = total.astype(rounded.dtype)
                copies.append(
                    pltpu.make_async_copy(
                        rounded.at[:, pl.ds(first, chunk)],
                        out_hbm.at[:, pl.ds(first, chunk)],
                        sent.at[first // chunk],
                    )
                )
                copies[-1].start()
            for copy in copies:
                copy.wait()

        for slots in ((0, 1), (0,), (1,), ()):
            wanted = [(sources[slot] >= 0) == (slot in slots) for slot in range(2)]

            @pl.when(wanted[0] & wanted[1])
            def _():
                finish(slots)

    vmem = pl.BlockSpec(memory_space=pltpu.VMEM)
    return pl.pallas_call(
        body,
        in_specs=[vmem] * 4,
        out_specs=pl.BlockSpec(memory_space=pl.ANY),
        out_shape=pltpu.HBM((rows, columns), jnp.bfloat16),
        scratch_shapes=[
            pltpu.VMEM((rows, columns), jnp.bfloat16),
            pltpu.SemaphoreType.DMA((columns // chunk,)),
        ],
        compiler_params=pltpu.CompilerParams(vmem_limit_bytes=16 << 20),
        name="late_product",
    )(merged, early_sum, *far_pieces)


def on_device(
    tokens,
    norm_gain,
    query_weight,
    key_weight,
    value_weight,
    sink_logits,
    conv_in_weight,
    conv_gate_weight,
    conv_taps,
    conv_gain,
    point_weight,
    output_gain,
    output_weight,
):
    sp_size, tp_size = lax.axis_size("sp"), lax.axis_size("tp")
    lines = sp_size // 2
    by_shares = sends_shares(sp_size, tp_size)
    if by_shares:
        routes = ShareRoutes(lines, tp_size)
        near = routes.send(output_weight, routes.beside)
        far = routes.send(output_weight, routes.beyond)
    *last_rows, tail, joined, other_tokens = project_last(
        tokens, norm_gain, query_weight, key_weight, value_weight, conv_in_weight, conv_gate_weight
    )
    earlier = from_behind(tail, "sp", 1)
    pair_width = key_weight.shape[1] + value_weight.shape[1]
    first_rows = project_rest(other_tokens, norm_gain, joined, query_weight.shape[1], pair_width)
    mixed = mix_rows(first_rows, last_rows, earlier, sink_logits, conv_taps, tp_size)
    exchanged = lax.all_to_all(mixed, "tp", split_axis=0, concat_axis=0, tiled=True)
    merged = merge_mixers(exchanged, conv_gain, point_weight, output_gain)
    if by_shares:
        near_across = routes.send(near, routes.holders_across)
        far_other = routes.send(far, routes.to_neighbours)
        near_pieces = near, routes.send(near, routes.lanes)
        near_pieces += near_across, routes.send(near_across, routes.lanes)
        far_pieces = far, routes.send(far, routes.lanes)
        last_pieces = far_other, routes.send(far_other, routes.lanes)
        early_sum = early_product(merged, output_weight, near_pieces, far_pieces, lines)
        return late_product(merged, early_sum, last_pieces, lines)
    projected = jnp.dot(
        merged,
        lax.all_gather(output_weight, "sp", axis=0, tiled=True),
        preferred_element_type=jnp.float32,
    )
    return projected.astype(jnp.bfloat16)


def sends_shares(sp_size, tp_size):
    return sp_size % 2 == 0 and tp_size % 4 == 0 and 3 <= sp_size // 2 <= 4


def solution(mesh):
    in_specs = (
        P("sp", None),
        P(),
        P(None, "tp"),
        P(None, "tp"),
        P(None, "tp"),
        P("tp"),
        P(None, "tp"),
        P(None, "tp"),
        P(),
        P(),
        P(),
        P(),
        P("sp", None),
    )
    out_specs = P(("sp", "tp"), None)
    return jax.shard_map(
        on_device, mesh=mesh, in_specs=in_specs, out_specs=out_specs, check_vma=False
    )
```

```python
import jax
import jax.numpy as jnp
from jax import lax
from jax.experimental import pallas as pl
from jax.experimental.pallas import tpu as pltpu
from jax.sharding import PartitionSpec as P


HEAD_DIM = 64
WINDOW = 128
CONV_WIDTH = 31


NORM_EPSILON = 1e-06
MASKED_SCORE = -1e30
HALO = 32


PLACE = ("sp", "tp")


def from_behind(block, axis, distance):
    devices = range(lax.axis_size(axis))
    route = [(i - distance, i) for i in devices if i - distance in devices]
    return lax.ppermute(block, axis, route)


BLOCK = 256


def normed_rows(token_rows, gain):
    widened = token_rows.astype(jnp.float32)
    scale = lax.rsqrt(jnp.mean(widened * widened, axis=-1, keepdims=True) + NORM_EPSILON)
    return (widened * scale * gain).astype(jnp.bfloat16)


def split_product(normed, joined, heads_width, pair_width, channels):
    result = jnp.dot(normed, joined, preferred_element_type=jnp.float32)
    pairs_end = heads_width + pair_width
    conv_in = result[:, pairs_end : pairs_end + channels]
    gated = conv_in * jax.nn.sigmoid(result[:, pairs_end + channels :])
    return [
        part.astype(jnp.bfloat16)
        for part in (result[:, :heads_width], result[:, heads_width:pairs_end], gated)
    ]


def project_last(tokens, norm_gain, query_weight, key_weight, value_weight, in_weight, gate_weight):
    rows, width = tokens.shape
    heads_width, key_width, channels = query_weight.shape[1], key_weight.shape[1], in_weight.shape[1]
    pair_width = key_width + value_weight.shape[1]
    tail = WINDOW + HALO
    others = rows - BLOCK
    starts = [0, heads_width + pair_width, heads_width + pair_width + channels]

    def body(
        gain_hbm, tokens_hbm, query_hbm, key_hbm, value_hbm, in_hbm, gate_hbm,
        queries_ref, pairs_ref, gated_ref, tail_ref, joined, rest_ref,
        last_ref, pairs_rows, gain_ref, arrived,
    ):
        copies = [
            pltpu.make_async_copy(source, target, arrived.at[i])
            for i, (source, target) in enumerate(
                [
                    (gain_hbm, gain_ref),
                    (tokens_hbm.at[pl.ds(others, BLOCK)], last_ref),
                    (key_hbm, pairs_rows.at[pl.ds(0, key_width)]),
                    (value_hbm, pairs_rows.at[pl.ds(key_width, pair_width - key_width)]),
                ]
                + [
                    (source, joined.at[:, pl.ds(start, source.shape[1])])
                    for source, start in zip([query_hbm, in_hbm, gate_hbm], starts)
                ]
                + [(tokens_hbm.at[pl.ds(0, others)], rest_ref)]
            )
        ]
        for copy in copies:
            copy.start()
        for copy in copies[:2]:
            copy.wait()
        normed = normed_rows(last_ref[...], gain_ref[...])
        for copy in copies[2:4]:
            copy.wait()
        joined[:, heads_width : heads_width + pair_width] = pairs_rows[...].T
        for copy in copies[4:7]:
            copy.wait()
        queries, pairs, gated = split_product(
            normed, joined[...], heads_width, pair_width, channels
        )
        queries_ref[...] = queries
        pairs_ref[...] = pairs
        gated_ref[...] = gated
        tail_ref[:WINDOW] = pairs[BLOCK - WINDOW :]
        tail_ref[WINDOW:] = gated[BLOCK - HALO :]
        copies[7].wait()

    vmem = pl.BlockSpec(memory_space=pltpu.VMEM)
    in_hbm = [
        pltpu.with_memory_space_constraint(operand, pltpu.HBM)
        for operand in (
            norm_gain[None], tokens, query_weight, key_weight.T, value_weight.T, in_weight,
            gate_weight,
        )
    ]
    shapes = [
        (BLOCK, heads_width), (BLOCK, pair_width), (BLOCK, channels), (tail, channels),
        (width, heads_width + pair_width + 2 * channels), (others, width),
    ]
    return pl.pallas_call(
        body,
        in_specs=[pl.BlockSpec(memory_space=pl.ANY)] * 7,
        out_specs=[vmem] * len(shapes),
        out_shape=[jax.ShapeDtypeStruct(shape, jnp.bfloat16) for shape in shapes[:4]]
        + [pltpu.VMEM(shape, jnp.bfloat16) for shape in shapes[4:]],
        scratch_shapes=[
            pltpu.VMEM((BLOCK, width), jnp.bfloat16),
            pltpu.VMEM((pair_width, width), jnp.bfloat16),
            pltpu.VMEM((1, width), jnp.float32),
            pltpu.SemaphoreType.DMA((8,)),
        ],
        compiler_params=pltpu.CompilerParams(vmem_limit_bytes=10 << 20),
        name="project_last",
    )(*in_hbm)


def project_rest(tokens, norm_gain, joined, heads_width, pair_width):
    rows, width = tokens.shape
    channels = (joined.shape[1] - heads_width - pair_width) // 2
    blocks = rows // BLOCK

    def body(gain_ref, tokens_ref, joined_ref, queries_ref, pairs_ref, gated_ref, normed):
        normed[0] = normed_rows(tokens_ref[:BLOCK], gain_ref[...])
        for i in range(blocks):
            here = slice(i * BLOCK, (i + 1) * BLOCK)
            queries, pairs, gated = split_product(
                normed[i], joined_ref[...], heads_width, pair_width, channels
            )
            if i + 1 < blocks:
                following = tokens_ref[(i + 1) * BLOCK : (i + 2) * BLOCK]
                normed[i + 1] = normed_rows(following, gain_ref[...])
            queries_ref[here] = queries
            pairs_ref[here] = pairs
            gated_ref[here] = gated

    vmem = pl.BlockSpec(memory_space=pltpu.VMEM)
    return pl.pallas_call(
        body,
        in_specs=[vmem] * 3,
        out_specs=[vmem] * 3,
        out_shape=[
            jax.ShapeDtypeStruct((rows, columns), jnp.bfloat16)
            for columns in (heads_width, pair_width, channels)
        ],
        scratch_shapes=[pltpu.VMEM((blocks, BLOCK, width), jnp.bfloat16)],
        compiler_params=pltpu.CompilerParams(vmem_limit_bytes=12 << 20),
        name="project_rest",
    )(
        norm_gain[None],
        pltpu.with_memory_space_constraint(tokens, pltpu.VMEM),
        pltpu.with_memory_space_constraint(joined, pltpu.VMEM),
    )


def mix_rows(first_rows, last_rows, earlier, sinks, taps, shares):
    rest, heads_width = first_rows[0].shape
    rows = rest + last_rows[0].shape[0]
    pair_width, channels = first_rows[1].shape[1], first_rows[2].shape[1]
    head_count = heads_width // HEAD_DIM
    share_rows = rows // shares

    def body(
        sinks_ref, queries_ref, pairs_ref, gated_ref, last_queries, last_pairs, last_gated,
        earlier_ref, taps_ref, out_ref, band, extended,
    ):
        band[:WINDOW] = earlier_ref[:WINDOW]
        band[WINDOW : WINDOW + rest] = pairs_ref[...]
        band[WINDOW + rest :] = last_pairs[...]
        extended[:HALO] = earlier_ref[WINDOW:].astype(jnp.float32)
        extended[HALO : HALO + rest] = gated_ref[...].astype(jnp.float32)
        extended[HALO + rest :] = last_gated[...].astype(jnp.float32)
        query_index = lax.broadcasted_iota(jnp.int32, (WINDOW, 2 * WINDOW), 0)
        key_index = lax.broadcasted_iota(jnp.int32, (WINDOW, 2 * WINDOW), 1)
        distance = WINDOW + query_index - key_index
        in_window = (distance >= 0) & (distance < WINDOW)
        not_before = in_window & ((lax.axis_index("sp") > 0) | (key_index >= WINDOW))
        own = pl.multiple_of(lax.axis_index("tp") * channels, channels)
        tap_rows = taps_ref[:, pl.ds(own, channels)].astype(jnp.float32)
        for block in range(rows // WINDOW):
            start = block * WINDOW
            share, inner = start // share_rows, start % share_rows
            keys = band[start : start + 2 * WINDOW, :HEAD_DIM]
            values = band[start : start + 2 * WINDOW, HEAD_DIM : 2 * HEAD_DIM]
            allowed = not_before if block == 0 else in_window
            found = []
            for head in range(head_count):
                source, at = (queries_ref, start) if start < rest else (last_queries, start - rest)
                here = source[at : at + WINDOW, head * HEAD_DIM : (head + 1) * HEAD_DIM]
                scores = lax.dot_general(
                    here, keys, (((1,), (1,)), ((), ())), preferred_element_type=jnp.float32
                ) * HEAD_DIM ** (-0.5)
                scores = jnp.where(allowed, scores, MASKED_SCORE)
                sink = sinks_ref[head]
                peak = jnp.maximum(jnp.max(scores, axis=-1, keepdims=True), sink)
                raised = jnp.exp(scores - peak)
                denominator = jnp.sum(raised, axis=-1, keepdims=True) + jnp.exp(sink - peak)
                weights = (raised * (1.0 / denominator)).astype(jnp.bfloat16)
                found.append(
                    jnp.dot(weights, values, preferred_element_type=jnp.float32).astype(jnp.bfloat16)
                )
            out_ref[share, inner : inner + WINDOW, :heads_width] = jnp.concatenate(found, axis=1)
            total = jnp.zeros((WINDOW, channels), jnp.float32)
            for tap in range(CONV_WIDTH):
                from_row = start + HALO - (CONV_WIDTH - 1) + tap
                total = total + tap_rows[tap : tap + 1] * extended[from_row : from_row + WINDOW]
            out_ref[share, inner : inner + WINDOW, heads_width:] = total.astype(jnp.bfloat16)

    whole = pl.BlockSpec(memory_space=pltpu.VMEM)
    scalars = pl.BlockSpec(memory_space=pltpu.SMEM)
    return pl.pallas_call(
        body,
        in_specs=[scalars] + [whole] * 8,
        out_specs=whole,
        out_shape=jax.ShapeDtypeStruct((shares, share_rows, heads_width + channels), jnp.bfloat16),
        scratch_shapes=[
            pltpu.VMEM((WINDOW + rows, pair_width), jnp.bfloat16),
            pltpu.VMEM((HALO + rows, channels), jnp.float32),
        ],
        compiler_params=pltpu.CompilerParams(vmem_limit_bytes=12 << 20),
        name="mix_rows",
    )(sinks, *first_rows, *last_rows, earlier, taps)


def merge_mixers(exchanged, conv_gain, point_weight, output_gain):
    shares, rows, joint = exchanged.shape
    heads_width = joint // 2
    width = shares * heads_width

    def body(exchanged_ref, conv_gain_ref, gain_ref, point_hbm, out_ref, point_ref, fetched):
        fetch = pltpu.make_async_copy(point_hbm, point_ref, fetched)
        fetch.start()
        attended = jnp.concatenate(
            [exchanged_ref[i, :, :heads_width] for i in range(shares)], axis=1
        ).astype(jnp.float32)
        convolved = jnp.concatenate(
            [exchanged_ref[i, :, heads_width:] for i in range(shares)], axis=1
        ).astype(jnp.float32)
        centered = convolved - jnp.mean(convolved, axis=-1, keepdims=True)
        scaled = (
            centered
            * lax.rsqrt(jnp.mean(centered * centered, axis=-1, keepdims=True) + NORM_EPSILON)
            * conv_gain_ref[...]
        )
        activated = (scaled * jax.nn.sigmoid(scaled)).astype(jnp.bfloat16)
        out_ref[:, :width] = (
            attended
            * lax.rsqrt(jnp.mean(attended * attended, axis=-1, keepdims=True) + NORM_EPSILON)
            * gain_ref[:, :width]
        ).astype(jnp.bfloat16)
        fetch.wait()
        pointwise = jnp.dot(activated, point_ref[...], preferred_element_type=jnp.float32)
        out_ref[:, width:] = (
            pointwise
            * lax.rsqrt(jnp.mean(pointwise * pointwise, axis=-1, keepdims=True) + NORM_EPSILON)
            * gain_ref[:, width:]
        ).astype(jnp.bfloat16)

    vmem = pl.BlockSpec(memory_space=pltpu.VMEM)
    return pl.pallas_call(
        body,
        in_specs=[vmem] * 3 + [pl.BlockSpec(memory_space=pl.ANY)],
        out_specs=vmem,
        out_shape=jax.ShapeDtypeStruct((rows, output_gain.shape[0]), jnp.bfloat16),
        scratch_shapes=[
            pltpu.VMEM(point_weight.shape, point_weight.dtype),
            pltpu.SemaphoreType.DMA(()),
        ],
        compiler_params=pltpu.CompilerParams(vmem_limit_bytes=12 << 20),
        name="merge_mixers",
    )(
        exchanged, conv_gain[None], output_gain[None],
        pltpu.with_memory_space_constraint(point_weight, pltpu.HBM),
    )


class ShareRoutes:
    def __init__(self, lines, tp_size):
        self.lines, self.tp_size = lines, tp_size

    def number(self, line, side, lane):
        return (line * 2 + side) * self.tp_size + lane

    def send(self, block, target):
        found = []
        for line in range(self.lines):
            for side in range(2):
                for lane in range(self.tp_size):
                    to = target(line, side, lane)
                    if 0 <= to[0] < self.lines:
                        found.append((self.number(line, side, lane), self.number(*to)))
        return lax.ppermute(block, PLACE, found)

    def beside(self, line, side, lane):
        to_line = line + 1 if lane % 2 == 0 else line - 1
        if 0 <= to_line < self.lines:
            return to_line, side, lane
        return line, 1 - side, lane ^ 1

    def relays(self, line, lane):
        return line + (lane & 1) == 2

    def beyond(self, line, side, lane):
        last = self.lines - 1
        row = lane - lane % 2
        if self.relays(line, lane):
            return (0 if line == 1 else last), side, row
        if 0 < line < last:
            return line, 1 - side, row + 1
        if lane % 2 == (0 if line == 0 else 1):
            return (2 if line == 0 else last - 2), side, row
        return last - line, (1 - side if lane // 2 % 2 else side), row + 1

    def holders_across(self, line, side, lane):
        from_line = line - 1 if lane % 2 == 0 else line + 1
        return (line if 0 <= from_line < self.lines else -1), 1 - side, lane

    def to_neighbours(self, line, side, lane):
        if lane % 2 == 0:
            return line, 1 - side, lane
        return (line if line in (0, self.lines - 1) else -1), side, lane ^ 2

    def lanes(self, line, side, lane):
        return line, side, lane ^ 1


def place_of_device():
    position = lax.axis_index("sp")
    return position >> 1, position & 1, lax.axis_index("tp") & 1


def columns_of(merged_ref, from_line, sides, share_rows):
    found = []
    for at_side in sides:
        start = pl.multiple_of((from_line * 2 + at_side) * share_rows, share_rows)
        found.append(merged_ref[:, pl.ds(start, share_rows)])
    return jnp.concatenate(found, axis=1)


def far_line(line, at_lane, lines):
    two_away = jnp.where(line < 2, line + 2, line - 2)
    at_end = (line == 0) | (line == lines - 1)
    return jnp.where(at_lane == 0, two_away, jnp.where(at_end, lines - 1 - line, -1))


def far_side(side, at_lane):
    return jnp.where((at_lane == 1) & (odd_row() == 1), 1 - side, side)


def odd_row():
    return lax.axis_index("tp") // 2 % 2


def early_product(merged, share, near_pieces, far_pieces, lines):
    rows, _ = merged.shape
    share_rows, columns = share.shape

    def body(merged_ref, share_ref, *refs):
        near_refs, far_refs, out_ref = refs[:4], refs[4:6], refs[6]
        line, side, lane = place_of_device()

        def product(from_line, sides, *parts):
            return jnp.dot(
                columns_of(merged_ref, from_line, sides, share_rows),
                jnp.concatenate(parts, axis=0),
                preferred_element_type=jnp.float32,
            )

        both_sides = (side, 1 - side)
        at_end = (line == 0) | (line == lines - 1)
        holder = jnp.where(line == 0, 0, 1)
        for which in range(2):
            held = holder == (lane, 1 - lane)[which]
            for ends, ref in ((True, near_refs[which]), (False, far_refs[which])):

                @pl.when(held & (at_end == ends))
                def _():
                    out_ref[...] = product(line, both_sides, share_ref[...], ref[...])

        for which in range(2):
            at_lane = (lane, 1 - lane)[which]
            from_line = line - 1 + 2 * at_lane

            @pl.when((from_line >= 0) & (from_line < lines))
            def _():
                out_ref[...] += product(
                    from_line, both_sides, near_refs[which][...], near_refs[2 + which][...]
                )

        for which in range(2):
            at_lane = (lane, 1 - lane)[which]
            from_line = far_line(line, at_lane, lines)

            @pl.when(from_line >= 0)
            def _():
                out_ref[...] += product(
                    from_line, (far_side(side, at_lane),), far_refs[which][...]
                )

    vmem = pl.BlockSpec(memory_space=pltpu.VMEM)
    return pl.pallas_call(
        body,
        in_specs=[vmem] * 8,
        out_specs=vmem,
        out_shape=jax.ShapeDtypeStruct((rows, columns), jnp.float32),
        compiler_params=pltpu.CompilerParams(vmem_limit_bytes=16 << 20),
        name="early_product",
    )(merged, share, *near_pieces, *far_pieces)


def late_product(merged, early_sum, far_pieces, lines):
    rows, _ = merged.shape
    share_rows, columns = far_pieces[0].shape
    chunk = 512

    def body(merged_ref, early_ref, *refs):
        far_refs, out_hbm, rounded, sent = refs[:2], refs[2], refs[3], refs[4]
        line, side, lane = place_of_device()
        sources = [far_line(line, lane, lines), far_line(line, 1 - lane, lines)]
        sides = [1 - far_side(side, lane), 1 - far_side(side, 1 - lane)]

        def finish(slots):
            if slots:
                left = [
                    columns_of(merged_ref, sources[slot], (sides[slot],), share_rows)
                    for slot in slots
                ]
                left = jnp.concatenate(left, axis=1)
            copies = []
            for first in range(0, columns, chunk):
                here = slice(first, first + chunk)
                total = early_ref[:, here]
                if slots:
                    right = jnp.concatenate([far_refs[slot][:, here] for slot in slots], axis=0)
                    total = total + jnp.dot(left, right, preferred_element_type=jnp.float32)
                rounded[:, here] = total.astype(rounded.dtype)
                copies.append(
                    pltpu.make_async_copy(
                        rounded.at[:, pl.ds(first, chunk)],
                        out_hbm.at[:, pl.ds(first, chunk)],
                        sent.at[first // chunk],
                    )
                )
                copies[-1].start()
            for copy in copies:
                copy.wait()

        for slots in ((0, 1), (0,), (1,), ()):
            wanted = [(sources[slot] >= 0) == (slot in slots) for slot in range(2)]

            @pl.when(wanted[0] & wanted[1])
            def _():
                finish(slots)

    vmem = pl.BlockSpec(memory_space=pltpu.VMEM)
    return pl.pallas_call(
        body,
        in_specs=[vmem] * 4,
        out_specs=pl.BlockSpec(memory_space=pl.ANY),
        out_shape=pltpu.HBM((rows, columns), jnp.bfloat16),
        scratch_shapes=[
            pltpu.VMEM((rows, columns), jnp.bfloat16),
            pltpu.SemaphoreType.DMA((columns // chunk,)),
        ],
        compiler_params=pltpu.CompilerParams(vmem_limit_bytes=16 << 20),
        name="late_product",
    )(merged, early_sum, *far_pieces)


def on_device(
    tokens,
    norm_gain,
    query_weight,
    key_weight,
    value_weight,
    sink_logits,
    conv_in_weight,
    conv_gate_weight,
    conv_taps,
    conv_gain,
    point_weight,
    output_gain,
    output_weight,
):
    sp_size, tp_size = lax.axis_size("sp"), lax.axis_size("tp")
    lines = sp_size // 2
    by_shares = sends_shares(sp_size, tp_size)
    if by_shares:
        routes = ShareRoutes(lines, tp_size)
        near = routes.send(output_weight, routes.beside)
        relays = routes.relays(lax.axis_index("sp") >> 1, lax.axis_index("tp"))
        norm_gain, relays = lax.optimization_barrier((norm_gain, relays))
        passed_on = jnp.where(relays, near, output_weight)
        far = routes.send(passed_on, routes.beyond)
    *last_rows, tail, joined, other_tokens = project_last(
        tokens, norm_gain, query_weight, key_weight, value_weight, conv_in_weight, conv_gate_weight
    )
    earlier = from_behind(tail, "sp", 1)
    pair_width = key_weight.shape[1] + value_weight.shape[1]
    first_rows = project_rest(other_tokens, norm_gain, joined, query_weight.shape[1], pair_width)
    mixed = mix_rows(first_rows, last_rows, earlier, sink_logits, conv_taps, tp_size)
    exchanged = lax.all_to_all(mixed, "tp", split_axis=0, concat_axis=0, tiled=True)
    merged = merge_mixers(exchanged, conv_gain, point_weight, output_gain)
    if by_shares:
        near_across = routes.send(near, routes.holders_across)
        far_other = routes.send(far, routes.to_neighbours)
        near_pieces = near, routes.send(near, routes.lanes)
        near_pieces += near_across, routes.send(near_across, routes.lanes)
        far_pieces = far, routes.send(far, routes.lanes)
        last_pieces = far_other, routes.send(far_other, routes.lanes)
        early_sum = early_product(merged, output_weight, near_pieces, far_pieces, lines)
        return late_product(merged, early_sum, last_pieces, lines)
    projected = jnp.dot(
        merged,
        lax.all_gather(output_weight, "sp", axis=0, tiled=True),
        preferred_element_type=jnp.float32,
    )
    return projected.astype(jnp.bfloat16)


def sends_shares(sp_size, tp_size):
    return sp_size == 2 * 4 and tp_size % 4 == 0


def solution(mesh):
    in_specs = (
        P("sp", None),
        P(),
        P(None, "tp"),
        P(None, "tp"),
        P(None, "tp"),
        P("tp"),
        P(None, "tp"),
        P(None, "tp"),
        P(),
        P(),
        P(),
        P(),
        P("sp", None),
    )
    out_specs = P(("sp", "tp"), None)
    return jax.shard_map(
        on_device, mesh=mesh, in_specs=in_specs, out_specs=out_specs, check_vma=False
    )
```

```python
import jax
import jax.numpy as jnp
from jax import lax
from jax.experimental import pallas as pl
from jax.experimental.pallas import tpu as pltpu
from jax.sharding import PartitionSpec as P


HEAD_DIM = 64
WINDOW = 128
CONV_WIDTH = 31


NORM_EPSILON = 1e-06
MASKED_SCORE = -1e30
HALO = 32


PLACE = ("sp", "tp")


def from_behind(block, axis, distance):
    devices = range(lax.axis_size(axis))
    route = [(i - distance, i) for i in devices if i - distance in devices]
    return lax.ppermute(block, axis, route)


BLOCK = 256


def normed_rows(token_rows, gain):
    widened = token_rows.astype(jnp.float32)
    scale = lax.rsqrt(jnp.mean(widened * widened, axis=-1, keepdims=True) + NORM_EPSILON)
    return (widened * scale * gain).astype(jnp.bfloat16)


def split_product(normed, joined, heads_width, pair_width, channels):
    result = jnp.dot(normed, joined, preferred_element_type=jnp.float32)
    pairs_end = heads_width + pair_width
    conv_in = result[:, pairs_end : pairs_end + channels]
    gated = conv_in * jax.nn.sigmoid(result[:, pairs_end + channels :])
    return [
        part.astype(jnp.bfloat16)
        for part in (result[:, :heads_width], result[:, heads_width:pairs_end], gated)
    ]


def project_last(tokens, norm_gain, query_weight, key_weight, value_weight, in_weight, gate_weight):
    rows, width = tokens.shape
    heads_width, key_width, channels = query_weight.shape[1], key_weight.shape[1], in_weight.shape[1]
    pair_width = key_width + value_weight.shape[1]
    tail = WINDOW + HALO
    others = rows - BLOCK
    starts = [0, heads_width + pair_width, heads_width + pair_width + channels]

    def body(
        gain_hbm, tokens_hbm, query_hbm, key_hbm, value_hbm, in_hbm, gate_hbm,
        queries_ref, pairs_ref, gated_ref, tail_ref, joined, rest_ref,
        last_ref, pairs_rows, gain_ref, arrived,
    ):
        copies = [
            pltpu.make_async_copy(source, target, arrived.at[i])
            for i, (source, target) in enumerate(
                [
                    (gain_hbm, gain_ref),
                    (tokens_hbm.at[pl.ds(others, BLOCK)], last_ref),
                    (key_hbm, pairs_rows.at[pl.ds(0, key_width)]),
                    (value_hbm, pairs_rows.at[pl.ds(key_width, pair_width - key_width)]),
                ]
                + [
                    (source, joined.at[:, pl.ds(start, source.shape[1])])
                    for source, start in zip([query_hbm, in_hbm, gate_hbm], starts)
                ]
                + [(tokens_hbm.at[pl.ds(0, others)], rest_ref)]
            )
        ]
        for copy in copies:
            copy.start()
        for copy in copies[:2]:
            copy.wait()
        normed = normed_rows(last_ref[...], gain_ref[...])
        for copy in copies[2:4]:
            copy.wait()
        joined[:, heads_width : heads_width + pair_width] = pairs_rows[...].T
        for copy in copies[4:7]:
            copy.wait()
        queries, pairs, gated = split_product(
            normed, joined[...], heads_width, pair_width, channels
        )
        queries_ref[...] = queries
        pairs_ref[...] = pairs
        gated_ref[...] = gated
        tail_ref[:WINDOW] = pairs[BLOCK - WINDOW :]
        tail_ref[WINDOW:] = gated[BLOCK - HALO :]
        copies[7].wait()

    vmem = pl.BlockSpec(memory_space=pltpu.VMEM)
    in_hbm = [
        pltpu.with_memory_space_constraint(operand, pltpu.HBM)
        for operand in (
            norm_gain[None], tokens, query_weight, key_weight.T, value_weight.T, in_weight,
            gate_weight,
        )
    ]
    shapes = [
        (BLOCK, heads_width), (BLOCK, pair_width), (BLOCK, channels), (tail, channels),
        (width, heads_width + pair_width + 2 * channels), (others, width),
    ]
    return pl.pallas_call(
        body,
        in_specs=[pl.BlockSpec(memory_space=pl.ANY)] * 7,
        out_specs=[vmem] * len(shapes),
        out_shape=[jax.ShapeDtypeStruct(shape, jnp.bfloat16) for shape in shapes[:4]]
        + [pltpu.VMEM(shape, jnp.bfloat16) for shape in shapes[4:]],
        scratch_shapes=[
            pltpu.VMEM((BLOCK, width), jnp.bfloat16),
            pltpu.VMEM((pair_width, width), jnp.bfloat16),
            pltpu.VMEM((1, width), jnp.float32),
            pltpu.SemaphoreType.DMA((8,)),
        ],
        compiler_params=pltpu.CompilerParams(vmem_limit_bytes=10 << 20),
        name="project_last",
    )(*in_hbm)


def project_rest(tokens, norm_gain, joined, heads_width, pair_width):
    rows, width = tokens.shape
    channels = (joined.shape[1] - heads_width - pair_width) // 2
    blocks = rows // BLOCK

    def body(gain_ref, tokens_ref, joined_ref, queries_ref, pairs_ref, gated_ref, normed):
        normed[0] = normed_rows(tokens_ref[:BLOCK], gain_ref[...])
        for i in range(blocks):
            here = slice(i * BLOCK, (i + 1) * BLOCK)
            queries, pairs, gated = split_product(
                normed[i], joined_ref[...], heads_width, pair_width, channels
            )
            if i + 1 < blocks:
                following = tokens_ref[(i + 1) * BLOCK : (i + 2) * BLOCK]
                normed[i + 1] = normed_rows(following, gain_ref[...])
            queries_ref[here] = queries
            pairs_ref[here] = pairs
            gated_ref[here] = gated

    vmem = pl.BlockSpec(memory_space=pltpu.VMEM)
    return pl.pallas_call(
        body,
        in_specs=[vmem] * 3,
        out_specs=[vmem] * 3,
        out_shape=[
            jax.ShapeDtypeStruct((rows, columns), jnp.bfloat16)
            for columns in (heads_width, pair_width, channels)
        ],
        scratch_shapes=[pltpu.VMEM((blocks, BLOCK, width), jnp.bfloat16)],
        compiler_params=pltpu.CompilerParams(vmem_limit_bytes=12 << 20),
        name="project_rest",
    )(
        norm_gain[None],
        pltpu.with_memory_space_constraint(tokens, pltpu.VMEM),
        pltpu.with_memory_space_constraint(joined, pltpu.VMEM),
    )


def mix_rows(first_rows, last_rows, earlier, sinks, taps, shares):
    rest, heads_width = first_rows[0].shape
    rows = rest + last_rows[0].shape[0]
    pair_width, channels = first_rows[1].shape[1], first_rows[2].shape[1]
    head_count = heads_width // HEAD_DIM
    share_rows = rows // shares

    def body(
        sinks_ref, queries_ref, pairs_ref, gated_ref, last_queries, last_pairs, last_gated,
        earlier_ref, taps_ref, out_hbm, out_ref, band, extended, sent,
    ):
        copies = [
            pltpu.make_async_copy(out_ref.at[i], out_hbm.at[i], sent.at[i]) for i in range(shares)
        ]
        band[:WINDOW] = earlier_ref[:WINDOW]
        band[WINDOW : WINDOW + rest] = pairs_ref[...]
        band[WINDOW + rest :] = last_pairs[...]
        extended[:HALO] = earlier_ref[WINDOW:].astype(jnp.float32)
        extended[HALO : HALO + rest] = gated_ref[...].astype(jnp.float32)
        extended[HALO + rest :] = last_gated[...].astype(jnp.float32)
        shape = (WINDOW, WINDOW)
        before = lax.broadcasted_iota(jnp.int32, shape, 1) > lax.broadcasted_iota(jnp.int32, shape, 0)
        nothing_before = before & (lax.axis_index("sp") == 0)
        own = pl.multiple_of(lax.axis_index("tp") * channels, channels)
        tap_rows = taps_ref[:, pl.ds(own, channels)].astype(jnp.float32)
        for block in range(rows // WINDOW):
            start = block * WINDOW
            share, inner = start // share_rows, start % share_rows
            keys = band[start : start + 2 * WINDOW, :HEAD_DIM]
            values = band[start : start + 2 * WINDOW, HEAD_DIM : 2 * HEAD_DIM]
            found = []
            for head in range(head_count):
                source, at = (queries_ref, start) if start < rest else (last_queries, start - rest)
                here = source[at : at + WINDOW, head * HEAD_DIM : (head + 1) * HEAD_DIM]
                both = lax.dot_general(
                    here, keys, (((1,), (1,)), ((), ())), preferred_element_type=jnp.float32
                )
                scores = jnp.where(before, both[:, :WINDOW], both[:, WINDOW:]) * HEAD_DIM ** (-0.5)
                if block == 0:
                    scores = jnp.where(nothing_before, MASKED_SCORE, scores)
                sink = sinks_ref[head]
                peak = jnp.maximum(jnp.max(scores, axis=-1, keepdims=True), sink)
                raised = jnp.exp(scores - peak)
                denominator = jnp.sum(raised, axis=-1, keepdims=True) + jnp.exp(sink - peak)
                weights = raised * (1.0 / denominator)
                placed = jnp.concatenate(
                    [jnp.where(before, weights, 0.0), jnp.where(before, 0.0, weights)], axis=1
                ).astype(jnp.bfloat16)
                found.append(
                    jnp.dot(placed, values, preferred_element_type=jnp.float32).astype(jnp.bfloat16)
                )
            out_ref[share, inner : inner + WINDOW, :heads_width] = jnp.concatenate(found, axis=1)
            total = jnp.zeros((WINDOW, channels), jnp.float32)
            for tap in range(CONV_WIDTH):
                from_row = start + HALO - (CONV_WIDTH - 1) + tap
                total = total + tap_rows[tap : tap + 1] * extended[from_row : from_row + WINDOW]
            out_ref[share, inner : inner + WINDOW, heads_width:] = total.astype(jnp.bfloat16)
            if inner + WINDOW == share_rows:
                copies[share].start()
        for copy in copies:
            copy.wait()

    whole = pl.BlockSpec(memory_space=pltpu.VMEM)
    scalars = pl.BlockSpec(memory_space=pltpu.SMEM)
    return pl.pallas_call(
        body,
        in_specs=[scalars] + [whole] * 8,
        out_specs=pl.BlockSpec(memory_space=pl.ANY),
        out_shape=pltpu.HBM((shares, share_rows, heads_width + channels), jnp.bfloat16),
        scratch_shapes=[
            pltpu.VMEM((shares, share_rows, heads_width + channels), jnp.bfloat16),
            pltpu.VMEM((WINDOW + rows, pair_width), jnp.bfloat16),
            pltpu.VMEM((HALO + rows, channels), jnp.float32),
            pltpu.SemaphoreType.DMA((shares,)),
        ],
        compiler_params=pltpu.CompilerParams(vmem_limit_bytes=12 << 20),
        name="mix_rows",
    )(sinks, *first_rows, *last_rows, earlier, taps)


def merge_mixers(exchanged, conv_gain, point_weight, output_gain):
    shares, rows, joint = exchanged.shape
    heads_width = joint // 2
    width = shares * heads_width

    def body(exchanged_ref, conv_gain_ref, gain_ref, point_hbm, out_ref, point_ref, fetched):
        fetch = pltpu.make_async_copy(point_hbm, point_ref, fetched)
        fetch.start()
        attended = jnp.concatenate(
            [exchanged_ref[i, :, :heads_width] for i in range(shares)], axis=1
        ).astype(jnp.float32)
        convolved = jnp.concatenate(
            [exchanged_ref[i, :, heads_width:] for i in range(shares)], axis=1
        ).astype(jnp.float32)
        centered = convolved - jnp.mean(convolved, axis=-1, keepdims=True)
        scaled = (
            centered
            * lax.rsqrt(jnp.mean(centered * centered, axis=-1, keepdims=True) + NORM_EPSILON)
            * conv_gain_ref[...]
        )
        activated = (scaled * jax.nn.sigmoid(scaled)).astype(jnp.bfloat16)
        out_ref[:, :width] = (
            attended
            * lax.rsqrt(jnp.mean(attended * attended, axis=-1, keepdims=True) + NORM_EPSILON)
            * gain_ref[:, :width]
        ).astype(jnp.bfloat16)
        fetch.wait()
        pointwise = jnp.dot(activated, point_ref[...], preferred_element_type=jnp.float32)
        out_ref[:, width:] = (
            pointwise
            * lax.rsqrt(jnp.mean(pointwise * pointwise, axis=-1, keepdims=True) + NORM_EPSILON)
            * gain_ref[:, width:]
        ).astype(jnp.bfloat16)

    vmem = pl.BlockSpec(memory_space=pltpu.VMEM)
    return pl.pallas_call(
        body,
        in_specs=[vmem] * 3 + [pl.BlockSpec(memory_space=pl.ANY)],
        out_specs=vmem,
        out_shape=jax.ShapeDtypeStruct((rows, output_gain.shape[0]), jnp.bfloat16),
        scratch_shapes=[
            pltpu.VMEM(point_weight.shape, point_weight.dtype),
            pltpu.SemaphoreType.DMA(()),
        ],
        compiler_params=pltpu.CompilerParams(vmem_limit_bytes=12 << 20),
        name="merge_mixers",
    )(
        exchanged, conv_gain[None], output_gain[None],
        pltpu.with_memory_space_constraint(point_weight, pltpu.HBM),
    )


class ShareRoutes:
    def __init__(self, lines, tp_size):
        self.lines, self.tp_size = lines, tp_size

    def number(self, line, side, lane):
        return (line * 2 + side) * self.tp_size + lane

    def send(self, block, target):
        found = []
        for line in range(self.lines):
            for side in range(2):
                for lane in range(self.tp_size):
                    to = target(line, side, lane)
                    if 0 <= to[0] < self.lines:
                        found.append((self.number(line, side, lane), self.number(*to)))
        return lax.ppermute(block, PLACE, found)

    def beside(self, line, side, lane):
        to_line = line + 1 if lane % 2 == 0 else line - 1
        if 0 <= to_line < self.lines:
            return to_line, side, lane
        return line, 1 - side, lane ^ 1

    def relays(self, line, lane):
        return line + (lane & 1) == 2

    def beyond(self, line, side, lane):
        last = self.lines - 1
        row = lane - lane % 2
        if self.relays(line, lane):
            return (0 if line == 1 else last), side, row
        if 0 < line < last:
            return line, 1 - side, row + 1
        if lane % 2 == (0 if line == 0 else 1):
            return (2 if line == 0 else last - 2), side, row
        return last - line, (1 - side if lane // 2 % 2 else side), row + 1

    def holders_across(self, line, side, lane):
        from_line = line - 1 if lane % 2 == 0 else line + 1
        return (line if 0 <= from_line < self.lines else -1), 1 - side, lane

    def to_neighbours(self, line, side, lane):
        if lane % 2 == 0:
            return line, 1 - side, lane
        return (line if line in (0, self.lines - 1) else -1), side, lane ^ 2

    def lanes(self, line, side, lane):
        return line, side, lane ^ 1


def place_of_device():
    position = lax.axis_index("sp")
    return position >> 1, position & 1, lax.axis_index("tp") & 1


def columns_of(merged_ref, from_line, sides, share_rows):
    found = []
    for at_side in sides:
        start = pl.multiple_of((from_line * 2 + at_side) * share_rows, share_rows)
        found.append(merged_ref[:, pl.ds(start, share_rows)])
    return jnp.concatenate(found, axis=1)


def far_line(line, at_lane, lines):
    two_away = jnp.where(line < 2, line + 2, line - 2)
    at_end = (line == 0) | (line == lines - 1)
    return jnp.where(at_lane == 0, two_away, jnp.where(at_end, lines - 1 - line, -1))


def far_side(side, at_lane):
    return jnp.where((at_lane == 1) & (odd_row() == 1), 1 - side, side)


def odd_row():
    return lax.axis_index("tp") // 2 % 2


def early_product(merged, share, near_pieces, far_pieces, lines):
    rows, _ = merged.shape
    share_rows, columns = share.shape

    def body(merged_ref, share_ref, *refs):
        near_refs, far_refs, out_ref = refs[:4], refs[4:6], refs[6]
        line, side, lane = place_of_device()

        both_sides = (side, 1 - side)

        def pieces_of(at_line, at_lane):
            at_end = at_line in (0, lines - 1)
            which_of = {at_lane: 0, 1 - at_lane: 1}
            holder = which_of[0 if at_line == 0 else 1]
            opposite = (near_refs if at_end else far_refs)[holder]
            found = [(at_line, both_sides, (share_ref, opposite))]
            for held_by, which in which_of.items():
                beside = at_line - 1 + 2 * held_by
                if 0 <= beside < lines:
                    found.append((beside, both_sides, (near_refs[which], near_refs[2 + which])))
                if held_by == 0 or at_end:
                    two_away = at_line + 2 if at_line < 2 else at_line - 2
                    beyond = two_away if held_by == 0 else lines - 1 - at_line
                    found.append((beyond, (far_side(side, held_by),), (far_refs[which],)))
            return found

        for at_line in range(lines):
            for at_lane in range(2):

                @pl.when((line == at_line) & (lane == at_lane))
                def _():
                    found = pieces_of(at_line, at_lane)
                    left = [
                        columns_of(merged_ref, from_line, sides, share_rows)
                        for from_line, sides, _ in found
                    ]
                    right = [ref[...] for _, _, refs_here in found for ref in refs_here]
                    out_ref[...] = jnp.dot(
                        jnp.concatenate(left, axis=1),
                        jnp.concatenate(right, axis=0),
                        preferred_element_type=jnp.float32,
                    )

    vmem = pl.BlockSpec(memory_space=pltpu.VMEM)
    return pl.pallas_call(
        body,
        in_specs=[vmem] * 8,
        out_specs=vmem,
        out_shape=jax.ShapeDtypeStruct((rows, columns), jnp.float32),
        compiler_params=pltpu.CompilerParams(vmem_limit_bytes=16 << 20),
        name="early_product",
    )(merged, share, *near_pieces, *far_pieces)


def late_product(merged, early_sum, far_pieces, lines):
    rows, _ = merged.shape
    share_rows, columns = far_pieces[0].shape
    chunk = 512

    def body(merged_ref, early_ref, *refs):
        far_refs, out_hbm, rounded, sent = refs[:2], refs[2], refs[3], refs[4]
        line, side, lane = place_of_device()
        sources = [far_line(line, lane, lines), far_line(line, 1 - lane, lines)]
        sides = [1 - far_side(side, lane), 1 - far_side(side, 1 - lane)]

        def finish(slots):
            if slots:
                left = [
                    columns_of(merged_ref, sources[slot], (sides[slot],), share_rows)
                    for slot in slots
                ]
                left = jnp.concatenate(left, axis=1)
            copies = []
            for first in range(0, columns, chunk):
                here = slice(first, first + chunk)
                total = early_ref[:, here]
                if slots:
                    right = jnp.concatenate([far_refs[slot][:, here] for slot in slots], axis=0)
                    total = total + jnp.dot(left, right, preferred_element_type=jnp.float32)
                rounded[:, here] = total.astype(rounded.dtype)
                copies.append(
                    pltpu.make_async_copy(
                        rounded.at[:, pl.ds(first, chunk)],
                        out_hbm.at[:, pl.ds(first, chunk)],
                        sent.at[first // chunk],
                    )
                )
                copies[-1].start()
            for copy in copies:
                copy.wait()

        for slots in ((0, 1), (0,), (1,), ()):
            wanted = [(sources[slot] >= 0) == (slot in slots) for slot in range(2)]

            @pl.when(wanted[0] & wanted[1])
            def _():
                finish(slots)

    vmem = pl.BlockSpec(memory_space=pltpu.VMEM)
    return pl.pallas_call(
        body,
        in_specs=[vmem] * 4,
        out_specs=pl.BlockSpec(memory_space=pl.ANY),
        out_shape=pltpu.HBM((rows, columns), jnp.bfloat16),
        scratch_shapes=[
            pltpu.VMEM((rows, columns), jnp.bfloat16),
            pltpu.SemaphoreType.DMA((columns // chunk,)),
        ],
        compiler_params=pltpu.CompilerParams(vmem_limit_bytes=16 << 20),
        name="late_product",
    )(merged, early_sum, *far_pieces)


def on_device(
    tokens,
    norm_gain,
    query_weight,
    key_weight,
    value_weight,
    sink_logits,
    conv_in_weight,
    conv_gate_weight,
    conv_taps,
    conv_gain,
    point_weight,
    output_gain,
    output_weight,
):
    sp_size, tp_size = lax.axis_size("sp"), lax.axis_size("tp")
    lines = sp_size // 2
    by_shares = sends_shares(sp_size, tp_size)
    if by_shares:
        routes = ShareRoutes(lines, tp_size)
        near = routes.send(output_weight, routes.beside)
        relays = routes.relays(lax.axis_index("sp") >> 1, lax.axis_index("tp"))
        norm_gain, relays = lax.optimization_barrier((norm_gain, relays))
        passed_on = jnp.where(relays, near, output_weight)
        far = routes.send(passed_on, routes.beyond)
    *last_rows, tail, joined, other_tokens = project_last(
        tokens, norm_gain, query_weight, key_weight, value_weight, conv_in_weight, conv_gate_weight
    )
    earlier = from_behind(tail, "sp", 1)
    pair_width = key_weight.shape[1] + value_weight.shape[1]
    first_rows = project_rest(other_tokens, norm_gain, joined, query_weight.shape[1], pair_width)
    mixed = mix_rows(first_rows, last_rows, earlier, sink_logits, conv_taps, tp_size)
    exchanged = lax.all_to_all(mixed, "tp", split_axis=0, concat_axis=0, tiled=True)
    merged = merge_mixers(exchanged, conv_gain, point_weight, output_gain)
    if by_shares:
        near_across = routes.send(near, routes.holders_across)
        far_other = routes.send(far, routes.to_neighbours)
        near_pieces = near, routes.send(near, routes.lanes)
        near_pieces += near_across, routes.send(near_across, routes.lanes)
        far_pieces = far, routes.send(far, routes.lanes)
        last_pieces = far_other, routes.send(far_other, routes.lanes)
        early_sum = early_product(merged, output_weight, near_pieces, far_pieces, lines)
        return late_product(merged, early_sum, last_pieces, lines)
    projected = jnp.dot(
        merged,
        lax.all_gather(output_weight, "sp", axis=0, tiled=True),
        preferred_element_type=jnp.float32,
    )
    return projected.astype(jnp.bfloat16)


def sends_shares(sp_size, tp_size):
    return sp_size == 2 * 4 and tp_size % 4 == 0


def solution(mesh):
    in_specs = (
        P("sp", None),
        P(),
        P(None, "tp"),
        P(None, "tp"),
        P(None, "tp"),
        P("tp"),
        P(None, "tp"),
        P(None, "tp"),
        P(),
        P(),
        P(),
        P(),
        P("sp", None),
    )
    out_specs = P(("sp", "tp"), None)
    return jax.shard_map(
        on_device, mesh=mesh, in_specs=in_specs, out_specs=out_specs, check_vma=False
    )
```

```python
import jax
import jax.numpy as jnp
from jax import lax
from jax.experimental import pallas as pl
from jax.experimental.pallas import tpu as pltpu
from jax.sharding import PartitionSpec as P


HEAD_DIM = 64
WINDOW = 128
CONV_WIDTH = 31


NORM_EPSILON = 1e-06
MASKED_SCORE = -1e30
HALO = 32


PLACE = ("sp", "tp")


def from_behind(block, axis, distance):
    devices = range(lax.axis_size(axis))
    route = [(i - distance, i) for i in devices if i - distance in devices]
    return lax.ppermute(block, axis, route)


BLOCK = 256


def normed_rows(token_rows, gain):
    widened = token_rows.astype(jnp.float32)
    scale = lax.rsqrt(jnp.mean(widened * widened, axis=-1, keepdims=True) + NORM_EPSILON)
    return (widened * scale * gain).astype(jnp.bfloat16)


def split_product(normed, joined, heads_width, pair_width, channels):
    result = jnp.dot(normed, joined, preferred_element_type=jnp.float32)
    pairs_end = heads_width + pair_width
    conv_in = result[:, pairs_end : pairs_end + channels]
    gated = conv_in * jax.nn.sigmoid(result[:, pairs_end + channels :])
    return [
        part.astype(jnp.bfloat16)
        for part in (result[:, :heads_width], result[:, heads_width:pairs_end], gated)
    ]


def project_last(tokens, norm_gain, query_weight, key_weight, value_weight, in_weight, gate_weight):
    rows, width = tokens.shape
    heads_width, key_width, channels = query_weight.shape[1], key_weight.shape[1], in_weight.shape[1]
    pair_width = key_width + value_weight.shape[1]
    tail = WINDOW + HALO
    others = rows - BLOCK
    starts = [0, heads_width + pair_width, heads_width + pair_width + channels]

    def body(
        gain_hbm, tokens_hbm, query_hbm, key_hbm, value_hbm, in_hbm, gate_hbm,
        queries_ref, pairs_ref, gated_ref, tail_ref, joined, rest_ref,
        last_ref, pairs_rows, gain_ref, arrived,
    ):
        copies = [
            pltpu.make_async_copy(source, target, arrived.at[i])
            for i, (source, target) in enumerate(
                [
                    (gain_hbm, gain_ref),
                    (tokens_hbm.at[pl.ds(others, BLOCK)], last_ref),
                    (key_hbm, pairs_rows.at[pl.ds(0, key_width)]),
                    (value_hbm, pairs_rows.at[pl.ds(key_width, pair_width - key_width)]),
                ]
                + [
                    (source, joined.at[:, pl.ds(start, source.shape[1])])
                    for source, start in zip([query_hbm, in_hbm, gate_hbm], starts)
                ]
                + [(tokens_hbm.at[pl.ds(0, others)], rest_ref)]
            )
        ]
        for copy in copies:
            copy.start()
        for copy in copies[:2]:
            copy.wait()
        normed = normed_rows(last_ref[...], gain_ref[...])
        for copy in copies[2:4]:
            copy.wait()
        joined[:, heads_width : heads_width + pair_width] = pairs_rows[...].T
        for copy in copies[4:7]:
            copy.wait()
        queries, pairs, gated = split_product(
            normed, joined[...], heads_width, pair_width, channels
        )
        queries_ref[...] = queries
        pairs_ref[...] = pairs
        gated_ref[...] = gated
        tail_ref[:WINDOW] = pairs[BLOCK - WINDOW :]
        tail_ref[WINDOW:] = gated[BLOCK - HALO :]
        copies[7].wait()

    vmem = pl.BlockSpec(memory_space=pltpu.VMEM)
    in_hbm = [
        pltpu.with_memory_space_constraint(operand, pltpu.HBM)
        for operand in (
            norm_gain[None], tokens, query_weight, key_weight.T, value_weight.T, in_weight,
            gate_weight,
        )
    ]
    shapes = [
        (BLOCK, heads_width), (BLOCK, pair_width), (BLOCK, channels), (tail, channels),
        (width, heads_width + pair_width + 2 * channels), (others, width),
    ]
    return pl.pallas_call(
        body,
        in_specs=[pl.BlockSpec(memory_space=pl.ANY)] * 7,
        out_specs=[vmem] * len(shapes),
        out_shape=[jax.ShapeDtypeStruct(shape, jnp.bfloat16) for shape in shapes[:4]]
        + [pltpu.VMEM(shape, jnp.bfloat16) for shape in shapes[4:]],
        scratch_shapes=[
            pltpu.VMEM((BLOCK, width), jnp.bfloat16),
            pltpu.VMEM((pair_width, width), jnp.bfloat16),
            pltpu.VMEM((1, width), jnp.float32),
            pltpu.SemaphoreType.DMA((8,)),
        ],
        compiler_params=pltpu.CompilerParams(vmem_limit_bytes=10 << 20),
        name="project_last",
    )(*in_hbm)


def project_rest(tokens, norm_gain, joined, heads_width, pair_width):
    rows, width = tokens.shape
    channels = (joined.shape[1] - heads_width - pair_width) // 2
    blocks = rows // BLOCK

    def body(gain_ref, tokens_ref, joined_ref, queries_ref, pairs_ref, gated_ref, normed):
        normed[0] = normed_rows(tokens_ref[:BLOCK], gain_ref[...])
        for i in range(blocks):
            here = slice(i * BLOCK, (i + 1) * BLOCK)
            queries, pairs, gated = split_product(
                normed[i], joined_ref[...], heads_width, pair_width, channels
            )
            if i + 1 < blocks:
                following = tokens_ref[(i + 1) * BLOCK : (i + 2) * BLOCK]
                normed[i + 1] = normed_rows(following, gain_ref[...])
            queries_ref[here] = queries
            pairs_ref[here] = pairs
            gated_ref[here] = gated

    vmem = pl.BlockSpec(memory_space=pltpu.VMEM)
    return pl.pallas_call(
        body,
        in_specs=[vmem] * 3,
        out_specs=[vmem] * 3,
        out_shape=[
            jax.ShapeDtypeStruct((rows, columns), jnp.bfloat16)
            for columns in (heads_width, pair_width, channels)
        ],
        scratch_shapes=[pltpu.VMEM((blocks, BLOCK, width), jnp.bfloat16)],
        compiler_params=pltpu.CompilerParams(vmem_limit_bytes=12 << 20),
        name="project_rest",
    )(
        norm_gain[None],
        pltpu.with_memory_space_constraint(tokens, pltpu.VMEM),
        pltpu.with_memory_space_constraint(joined, pltpu.VMEM),
    )


def mix_rows(first_rows, last_rows, earlier, sinks, taps, shares):
    rest, heads_width = first_rows[0].shape
    rows = rest + last_rows[0].shape[0]
    pair_width, channels = first_rows[1].shape[1], first_rows[2].shape[1]
    head_count = heads_width // HEAD_DIM
    share_rows = rows // shares

    def body(
        sinks_ref, queries_ref, pairs_ref, gated_ref, last_queries, last_pairs, last_gated,
        earlier_ref, taps_ref, out_hbm, out_ref, band, extended, sent,
    ):
        copies = [
            pltpu.make_async_copy(out_ref.at[i], out_hbm.at[i], sent.at[i]) for i in range(shares)
        ]
        band[:WINDOW] = earlier_ref[:WINDOW]
        band[WINDOW : WINDOW + rest] = pairs_ref[...]
        band[WINDOW + rest :] = last_pairs[...]
        extended[:HALO] = earlier_ref[WINDOW:].astype(jnp.float32)
        extended[HALO : HALO + rest] = gated_ref[...].astype(jnp.float32)
        extended[HALO + rest :] = last_gated[...].astype(jnp.float32)
        shape = (WINDOW, WINDOW)
        before = lax.broadcasted_iota(jnp.int32, shape, 1) > lax.broadcasted_iota(jnp.int32, shape, 0)
        nothing_before = before & (lax.axis_index("sp") == 0)
        own = pl.multiple_of(lax.axis_index("tp") * channels, channels)
        tap_rows = taps_ref[:, pl.ds(own, channels)].astype(jnp.float32)
        for block in range(rows // WINDOW):
            start = block * WINDOW
            share, inner = start // share_rows, start % share_rows
            keys = band[start : start + 2 * WINDOW, :HEAD_DIM]
            values = band[start : start + 2 * WINDOW, HEAD_DIM : 2 * HEAD_DIM]
            found = []
            for head in range(head_count):
                source, at = (queries_ref, start) if start < rest else (last_queries, start - rest)
                here = source[at : at + WINDOW, head * HEAD_DIM : (head + 1) * HEAD_DIM]
                both = lax.dot_general(
                    here, keys, (((1,), (1,)), ((), ())), preferred_element_type=jnp.float32
                )
                scores = jnp.where(before, both[:, :WINDOW], both[:, WINDOW:]) * HEAD_DIM ** (-0.5)
                if block == 0:
                    scores = jnp.where(nothing_before, MASKED_SCORE, scores)
                sink = sinks_ref[head]
                peak = jnp.maximum(jnp.max(scores, axis=-1, keepdims=True), sink)
                raised = jnp.exp(scores - peak)
                denominator = jnp.sum(raised, axis=-1, keepdims=True) + jnp.exp(sink - peak)
                weights = raised * (1.0 / denominator)
                placed = jnp.concatenate(
                    [jnp.where(before, weights, 0.0), jnp.where(before, 0.0, weights)], axis=1
                ).astype(jnp.bfloat16)
                found.append(
                    jnp.dot(placed, values, preferred_element_type=jnp.float32).astype(jnp.bfloat16)
                )
            out_ref[share, inner : inner + WINDOW, :heads_width] = jnp.concatenate(found, axis=1)
            total = jnp.zeros((WINDOW, channels), jnp.float32)
            for tap in range(CONV_WIDTH):
                from_row = start + HALO - (CONV_WIDTH - 1) + tap
                total = total + tap_rows[tap : tap + 1] * extended[from_row : from_row + WINDOW]
            out_ref[share, inner : inner + WINDOW, heads_width:] = total.astype(jnp.bfloat16)
            if inner + WINDOW == share_rows:
                copies[share].start()
        for copy in copies:
            copy.wait()

    whole = pl.BlockSpec(memory_space=pltpu.VMEM)
    scalars = pl.BlockSpec(memory_space=pltpu.SMEM)
    return pl.pallas_call(
        body,
        in_specs=[scalars] + [whole] * 8,
        out_specs=pl.BlockSpec(memory_space=pl.ANY),
        out_shape=pltpu.HBM((shares, share_rows, heads_width + channels), jnp.bfloat16),
        scratch_shapes=[
            pltpu.VMEM((shares, share_rows, heads_width + channels), jnp.bfloat16),
            pltpu.VMEM((WINDOW + rows, pair_width), jnp.bfloat16),
            pltpu.VMEM((HALO + rows, channels), jnp.float32),
            pltpu.SemaphoreType.DMA((shares,)),
        ],
        compiler_params=pltpu.CompilerParams(vmem_limit_bytes=12 << 20),
        name="mix_rows",
    )(sinks, *first_rows, *last_rows, earlier, taps)


def fetched(weight):
    def body(weight_hbm, out_ref, moved):
        copy = pltpu.make_async_copy(weight_hbm, out_ref, moved)
        copy.start()
        copy.wait()

    return pl.pallas_call(
        body,
        in_specs=[pl.BlockSpec(memory_space=pl.ANY)],
        out_specs=pl.BlockSpec(memory_space=pltpu.VMEM),
        out_shape=jax.ShapeDtypeStruct(weight.shape, weight.dtype),
        scratch_shapes=[pltpu.SemaphoreType.DMA(())],
        compiler_params=pltpu.CompilerParams(vmem_limit_bytes=4 << 20),
        name="fetched",
    )(pltpu.with_memory_space_constraint(weight, pltpu.HBM))


def merge_mixers(exchanged, conv_gain, point_weight, output_gain):
    shares, rows, joint = exchanged.shape
    heads_width = joint // 2
    width = shares * heads_width

    def body(exchanged_ref, conv_gain_ref, gain_ref, point_ref, out_ref):
        attended = jnp.concatenate(
            [exchanged_ref[i, :, :heads_width] for i in range(shares)], axis=1
        ).astype(jnp.float32)
        convolved = jnp.concatenate(
            [exchanged_ref[i, :, heads_width:] for i in range(shares)], axis=1
        ).astype(jnp.float32)
        centered = convolved - jnp.mean(convolved, axis=-1, keepdims=True)
        scaled = (
            centered
            * lax.rsqrt(jnp.mean(centered * centered, axis=-1, keepdims=True) + NORM_EPSILON)
            * conv_gain_ref[...]
        )
        activated = (scaled * jax.nn.sigmoid(scaled)).astype(jnp.bfloat16)
        out_ref[:, :width] = (
            attended
            * lax.rsqrt(jnp.mean(attended * attended, axis=-1, keepdims=True) + NORM_EPSILON)
            * gain_ref[:, :width]
        ).astype(jnp.bfloat16)
        pointwise = jnp.dot(activated, point_ref[...], preferred_element_type=jnp.float32)
        out_ref[:, width:] = (
            pointwise
            * lax.rsqrt(jnp.mean(pointwise * pointwise, axis=-1, keepdims=True) + NORM_EPSILON)
            * gain_ref[:, width:]
        ).astype(jnp.bfloat16)

    vmem = pl.BlockSpec(memory_space=pltpu.VMEM)
    return pl.pallas_call(
        body,
        in_specs=[vmem] * 4,
        out_specs=vmem,
        out_shape=jax.ShapeDtypeStruct((rows, output_gain.shape[0]), jnp.bfloat16),
        compiler_params=pltpu.CompilerParams(vmem_limit_bytes=12 << 20),
        name="merge_mixers",
    )(exchanged, conv_gain[None], output_gain[None], point_weight)


class ShareRoutes:
    def __init__(self, lines, tp_size):
        self.lines, self.tp_size = lines, tp_size

    def number(self, line, side, lane):
        return (line * 2 + side) * self.tp_size + lane

    def send(self, block, target):
        found = []
        for line in range(self.lines):
            for side in range(2):
                for lane in range(self.tp_size):
                    to = target(line, side, lane)
                    if 0 <= to[0] < self.lines:
                        found.append((self.number(line, side, lane), self.number(*to)))
        return lax.ppermute(block, PLACE, found)

    def beside(self, line, side, lane):
        to_line = line + 1 if lane % 2 == 0 else line - 1
        if 0 <= to_line < self.lines:
            return to_line, side, lane
        return line, 1 - side, lane ^ 1

    def relays(self, line, lane):
        return line + (lane & 1) == 2

    def beyond(self, line, side, lane):
        last = self.lines - 1
        row = lane - lane % 2
        if self.relays(line, lane):
            return (0 if line == 1 else last), side, row
        if 0 < line < last:
            return line, 1 - side, row + 1
        if lane % 2 == (0 if line == 0 else 1):
            return (2 if line == 0 else last - 2), side, row
        return last - line, (1 - side if lane // 2 % 2 else side), row + 1

    def holders_across(self, line, side, lane):
        from_line = line - 1 if lane % 2 == 0 else line + 1
        return (line if 0 <= from_line < self.lines else -1), 1 - side, lane

    def to_neighbours(self, line, side, lane):
        if lane % 2 == 0:
            return line, 1 - side, lane
        return (line if line in (0, self.lines - 1) else -1), side, lane ^ 2

    def lanes(self, line, side, lane):
        return line, side, lane ^ 1


def place_of_device():
    position = lax.axis_index("sp")
    return position >> 1, position & 1, lax.axis_index("tp") & 1


def columns_of(merged_ref, from_line, sides, share_rows):
    found = []
    for at_side in sides:
        start = pl.multiple_of((from_line * 2 + at_side) * share_rows, share_rows)
        found.append(merged_ref[:, pl.ds(start, share_rows)])
    return jnp.concatenate(found, axis=1)


def far_line(line, at_lane, lines):
    two_away = jnp.where(line < 2, line + 2, line - 2)
    at_end = (line == 0) | (line == lines - 1)
    return jnp.where(at_lane == 0, two_away, jnp.where(at_end, lines - 1 - line, -1))


def far_side(side, at_lane):
    return jnp.where((at_lane == 1) & (odd_row() == 1), 1 - side, side)


def odd_row():
    return lax.axis_index("tp") // 2 % 2


def early_product(merged, share, near_pieces, far_pieces, lines):
    rows, _ = merged.shape
    share_rows, columns = share.shape

    def body(merged_ref, share_ref, *refs):
        near_refs, far_refs, out_ref = refs[:4], refs[4:6], refs[6]
        line, side, lane = place_of_device()

        both_sides = (side, 1 - side)

        def pieces_of(at_line, at_lane):
            at_end = at_line in (0, lines - 1)
            which_of = {at_lane: 0, 1 - at_lane: 1}
            holder = which_of[0 if at_line == 0 else 1]
            opposite = (near_refs if at_end else far_refs)[holder]
            found = [(at_line, both_sides, (share_ref, opposite))]
            for held_by, which in which_of.items():
                beside = at_line - 1 + 2 * held_by
                if 0 <= beside < lines:
                    found.append((beside, both_sides, (near_refs[which], near_refs[2 + which])))
                if held_by == 0 or at_end:
                    two_away = at_line + 2 if at_line < 2 else at_line - 2
                    beyond = two_away if held_by == 0 else lines - 1 - at_line
                    found.append((beyond, (far_side(side, held_by),), (far_refs[which],)))
            return found

        for at_line in range(lines):
            for at_lane in range(2):

                @pl.when((line == at_line) & (lane == at_lane))
                def _():
                    found = pieces_of(at_line, at_lane)
                    left = [
                        columns_of(merged_ref, from_line, sides, share_rows)
                        for from_line, sides, _ in found
                    ]
                    right = [ref[...] for _, _, refs_here in found for ref in refs_here]
                    out_ref[...] = jnp.dot(
                        jnp.concatenate(left, axis=1),
                        jnp.concatenate(right, axis=0),
                        preferred_element_type=jnp.float32,
                    )

    vmem = pl.BlockSpec(memory_space=pltpu.VMEM)
    return pl.pallas_call(
        body,
        in_specs=[vmem] * 8,
        out_specs=vmem,
        out_shape=jax.ShapeDtypeStruct((rows, columns), jnp.float32),
        compiler_params=pltpu.CompilerParams(vmem_limit_bytes=16 << 20),
        name="early_product",
    )(merged, share, *near_pieces, *far_pieces)


def late_product(merged, early_sum, far_pieces, lines):
    rows, _ = merged.shape
    share_rows, columns = far_pieces[0].shape
    chunk = 512

    def body(merged_ref, early_ref, *refs):
        far_refs, out_hbm, rounded, sent = refs[:2], refs[2], refs[3], refs[4]
        line, side, lane = place_of_device()
        sources = [far_line(line, lane, lines), far_line(line, 1 - lane, lines)]
        sides = [1 - far_side(side, lane), 1 - far_side(side, 1 - lane)]

        def finish(slots):
            if slots:
                left = [
                    columns_of(merged_ref, sources[slot], (sides[slot],), share_rows)
                    for slot in slots
                ]
                left = jnp.concatenate(left, axis=1)
            copies = []
            for first in range(0, columns, chunk):
                here = slice(first, first + chunk)
                total = early_ref[:, here]
                if slots:
                    right = jnp.concatenate([far_refs[slot][:, here] for slot in slots], axis=0)
                    total = total + jnp.dot(left, right, preferred_element_type=jnp.float32)
                rounded[:, here] = total.astype(rounded.dtype)
                copies.append(
                    pltpu.make_async_copy(
                        rounded.at[:, pl.ds(first, chunk)],
                        out_hbm.at[:, pl.ds(first, chunk)],
                        sent.at[first // chunk],
                    )
                )
                copies[-1].start()
            for copy in copies:
                copy.wait()

        for slots in ((0, 1), (0,), (1,), ()):
            wanted = [(sources[slot] >= 0) == (slot in slots) for slot in range(2)]

            @pl.when(wanted[0] & wanted[1])
            def _():
                finish(slots)

    vmem = pl.BlockSpec(memory_space=pltpu.VMEM)
    return pl.pallas_call(
        body,
        in_specs=[vmem] * 4,
        out_specs=pl.BlockSpec(memory_space=pl.ANY),
        out_shape=pltpu.HBM((rows, columns), jnp.bfloat16),
        scratch_shapes=[
            pltpu.VMEM((rows, columns), jnp.bfloat16),
            pltpu.SemaphoreType.DMA((columns // chunk,)),
        ],
        compiler_params=pltpu.CompilerParams(vmem_limit_bytes=16 << 20),
        name="late_product",
    )(merged, early_sum, *far_pieces)


def on_device(
    tokens,
    norm_gain,
    query_weight,
    key_weight,
    value_weight,
    sink_logits,
    conv_in_weight,
    conv_gate_weight,
    conv_taps,
    conv_gain,
    point_weight,
    output_gain,
    output_weight,
):
    sp_size, tp_size = lax.axis_size("sp"), lax.axis_size("tp")
    lines = sp_size // 2
    by_shares = sends_shares(sp_size, tp_size)
    if by_shares:
        routes = ShareRoutes(lines, tp_size)
        near = routes.send(output_weight, routes.beside)
        relays = routes.relays(lax.axis_index("sp") >> 1, lax.axis_index("tp"))
        norm_gain, relays = lax.optimization_barrier((norm_gain, relays))
        passed_on = jnp.where(relays, near, output_weight)
        far = routes.send(passed_on, routes.beyond)
    *last_rows, tail, joined, other_tokens = project_last(
        tokens, norm_gain, query_weight, key_weight, value_weight, conv_in_weight, conv_gate_weight
    )
    earlier = from_behind(tail, "sp", 1)
    pair_width = key_weight.shape[1] + value_weight.shape[1]
    first_rows = project_rest(other_tokens, norm_gain, joined, query_weight.shape[1], pair_width)
    mixed = mix_rows(first_rows, last_rows, earlier, sink_logits, conv_taps, tp_size)
    exchanged = lax.all_to_all(mixed, "tp", split_axis=0, concat_axis=0, tiled=True)
    point_here = fetched(point_weight)
    merged = merge_mixers(exchanged, conv_gain, point_here, output_gain)
    if by_shares:
        near_across = routes.send(near, routes.holders_across)
        far_other = routes.send(far, routes.to_neighbours)
        near_pieces = near, routes.send(near, routes.lanes)
        near_pieces += near_across, routes.send(near_across, routes.lanes)
        far_pieces = far, routes.send(far, routes.lanes)
        last_pieces = far_other, routes.send(far_other, routes.lanes)
        early_sum = early_product(merged, output_weight, near_pieces, far_pieces, lines)
        return late_product(merged, early_sum, last_pieces, lines)
    projected = jnp.dot(
        merged,
        lax.all_gather(output_weight, "sp", axis=0, tiled=True),
        preferred_element_type=jnp.float32,
    )
    return projected.astype(jnp.bfloat16)


def sends_shares(sp_size, tp_size):
    return sp_size == 2 * 4 and tp_size % 4 == 0


def solution(mesh):
    in_specs = (
        P("sp", None),
        P(),
        P(None, "tp"),
        P(None, "tp"),
        P(None, "tp"),
        P("tp"),
        P(None, "tp"),
        P(None, "tp"),
        P(),
        P(),
        P(),
        P(),
        P("sp", None),
    )
    out_specs = P(("sp", "tp"), None)
    return jax.shard_map(
        on_device, mesh=mesh, in_specs=in_specs, out_specs=out_specs, check_vma=False
    )
```
